32 devices in a mesh: ep: 8 (over z, x), tp: 4 (over y, core).
Axes of the slice: x: 2, y: 2, z: 4, core: 2. Of those that a mesh axis runs over, the one named last changes fastest.
Arguments:
- tokens: bfloat16 [4096, 2048], P(('ep', 'tp')), may hold values from -6 to 6
- expert_ids: int32 [4096, 4], P(('ep', 'tp')), may hold values from 0 to 7, all different within a row; in each aligned block of 128 rows (0 to 127, 128 to 255, ...) at most 96 rows name the same one
- route_weights: float32 [4096, 4], P(('ep', 'tp')), may hold values from 0.2 to 1.2
- cotangent: bfloat16 [4096, 2048], P(('ep', 'tp')), may hold values from -6 to 6
- gate_weight: bfloat16 [32, 512, 2048], P(('ep', 'tp')), may hold values from -0.125 to 0.125
- up_weight: bfloat16 [32, 512, 2048], P(('ep', 'tp')), may hold values from -0.125 to 0.125
- down_weight: bfloat16 [32, 512, 2048], P(('ep', 'tp')), may hold values from -0.25 to 0.25
- shared_gate: bfloat16 [256, 2048], replicated, may hold values from -0.125 to 0.125
- shared_up: bfloat16 [256, 2048], replicated, may hold values from -0.125 to 0.125
- shared_down: bfloat16 [256, 2048], replicated, may hold values from -0.375 to 0.375
Outputs:
- token_grad: bfloat16 [4096, 2048], P(('ep', 'tp'))
- route_grad: float32 [4096, 4], P(('ep', 'tp'))
- gate_grad: bfloat16 [32, 512, 2048], P(('ep', 'tp'))
- up_grad: bfloat16 [32, 512, 2048], P(('ep', 'tp'))
- down_grad: bfloat16 [32, 512, 2048], P(('ep', 'tp'))
- shared_grads: float32 [2048, 3, 256], P(('ep', 'tp'))
The draws below stay inside these ranges and needn't reach their ends.
Inputs may be any that keep to these rules, and one draw needn't show every extreme that they name: `expert_ids`: each row names 4 different numbers of 0 to 7, experts within the group of the row's device. Among the rows of one device (aligned blocks of 128 tokens) no number is named more than 96 times, and in some blocks one number is named exactly 96 times.
All inputs are finite; a program needn't handle non-finite values.
Results may differ from the reference program's by a relative error of at most 0.006.
Values may be sent and summed in bfloat16 or wider, within the bound.
A program may use at most 128 MiB of HBM per device.

```python
import math
import jax
import jax.numpy as jnp
import numpy as np
from jax import lax

D = 2048
D_EXPERT = 512
D_SHARED = 256
TOP = 4
TOK_DEV = 128
GROUPS = 4
EXP_GROUP = 8
EXPERTS = 32
CAP = 96
TOKENS = 4096


def with_spikes(array, key, source, target, shards_of, factor):
    owner, partner = [(jnp.arange(array.shape[dim]) // (array.shape[dim] // shards_of)).reshape([-1 if axis == dim else 1 for axis in range(array.ndim)]) for dim in (source, target)]
    chosen = jax.random.permutation(key, shards_of)[partner]
    strong = (owner == chosen) | (owner == (partner + shards_of // 2) % shards_of)
    return jnp.where(strong, factor * array, array)


def level_of(key, extent, cuts, smallest, high):
    factor_of = 1.0
    for axis_at, parts in cuts:
        heights = jax.random.uniform(jax.random.fold_in(jax.random.fold_in(key, 6), axis_at), (parts,), jnp.float32, smallest / len(cuts), high / len(cuts))
        factor_of = factor_of * jnp.repeat(jnp.exp(heights), extent[axis_at] // parts).reshape((-1,) + (1,) * (len(extent) - 1 - axis_at))
    return factor_of


def routed_block(stream_key, own, number, rows, amount, top, most, skew):
    sequence = jax.random.permutation(stream_key, amount)
    packed, usual = load_shares(amount, rows * top, most, skew, True), load_shares(amount, rows * top, most, skew, False)
    places = jnp.arange(amount)

    def named(sizes, turn):
        used = int((sizes > 0).sum())
        fixed = max(1, used // 4)
        shifted = fixed + (places - fixed + turn * (used - fixed)) % max(1, amount - fixed)
        return jnp.zeros((amount,), jnp.int32).at[sequence[jnp.where(places < fixed, places, shifted)]].set(jnp.asarray(sizes, jnp.int32))

    sizes = jnp.where(number % 4 == 0, named(packed, number // 4), named(usual, number - number // 4 - 1))
    mixed = jax.random.permutation(jax.random.fold_in(own, 3), amount)
    giver, taker = mixed[0:amount // 2 * 2:2], mixed[1:amount // 2 * 2:2]
    slack = jnp.minimum(sizes[giver] - 1, most - sizes[taker]) // 2
    slack = jnp.where((giver == sequence[0]) | (taker == sequence[0]) | (sizes[taker] == 0), 0, jnp.maximum(slack, 0))
    shifted = jax.random.randint(jax.random.fold_in(own, 4), (amount // 2,), 0, 1 << 20) % (slack + 1)
    sizes = sizes.at[giver].add(-shifted).at[taker].add(shifted)
    labels = jnp.searchsorted(jnp.cumsum(sizes), jnp.arange(rows * top), side="right").astype(jnp.int32)
    listing = labels.reshape(top, rows).T
    listing = listing[jax.random.permutation(jax.random.fold_in(own, 1), rows)]
    turn = jax.random.randint(jax.random.fold_in(own, 2), (rows, 1), 0, top)
    return jnp.take_along_axis(listing, (jnp.arange(top)[None, :] + turn) % top, axis=1)


def load_shares(count, total, bound, lean, full):
    weights = [(1 << 20) // math.isqrt(grade ** lean) + 1 for grade in range(1, count + 1)]
    largest = bound if full else min(bound, max(-(-total // count), total * weights[0] // sum(weights)))
    least = 1 if total - largest >= count - 1 else 0
    given, surplus = [largest] + [least] * (count - 1), total - largest - least * (count - 1)
    while surplus > 0:
        free = [i for i in range(1, count) if given[i] < largest] or [i for i in range(1, count) if given[i] < bound]
        whole, budget = sum([weights[i] for i in free]), surplus
        for i in free:
            more = min(bound - given[i], max(1, budget * weights[i] // whole), surplus)
            given[i] = given[i] + more
            surplus = surplus - more
    return np.array(given)


def gaussian(own_key, dims, spread, most, pieces=(), kind=jnp.bfloat16):
    drawn = jax.random.normal(own_key, dims, jnp.float32) * spread
    if len(pieces) > 0:
        drawn = level_of(own_key, dims, pieces, -0.22, 0.18) * drawn
    return jnp.clip(drawn, min=-most, max=most).astype(kind)


def gaussian_with(rng, dims, width, most, pieces, heavy, held_as=jnp.bfloat16):
    values = width * jax.random.normal(rng, dims, jnp.float32)
    if pieces:
        values = values * level_of(rng, dims, pieces, -0.22, 0.18)
    return jnp.clip(with_spikes(values, jax.random.fold_in(rng, 3), *heavy), -most, most).astype(held_as)


def setup_inputs(seed: int = 0) -> dict:
    key_of = jax.random.split(jax.random.key(seed), 11)
    tokens = gaussian_with(key_of[0], (TOKENS, D), 1.0, 6.0, ((0, 32),), (0, 1, 32, 2.75))
    expert_ids_keys = jax.random.split(jax.random.fold_in(key_of[1], 1), TOKENS // TOK_DEV)
    expert_ids_turns = jax.random.permutation(jax.random.fold_in(key_of[1], 3), TOKENS // TOK_DEV)
    expert_ids = jax.vmap(lambda own, number: routed_block(jax.random.fold_in(key_of[1], 2), own, number, TOK_DEV, EXP_GROUP, TOP, CAP, 2))(expert_ids_keys, expert_ids_turns).reshape((TOKENS, TOP))
    route_weights = jnp.clip(0.2 + 1 * jax.random.uniform(key_of[2], (TOKENS, TOP), jnp.float32) ** level_of(key_of[2], (TOKENS, TOP), ((0, 32),), -0.2, 0.2), 0.2, 1.2)
    cotangent = gaussian_with(key_of[3], (TOKENS, D), 1.0, 6.0, ((0, 32),), (0, 1, 32, 2.75))
    gate_weight = gaussian(key_of[4], (EXPERTS, D_EXPERT, D), D ** -0.5, 0.125, ((0, 32),))
    up_weight = gaussian(key_of[5], (EXPERTS, D_EXPERT, D), D ** -0.5, 0.125, ((0, 32),))
    down_weight = gaussian(key_of[6], (EXPERTS, D_EXPERT, D), D_EXPERT ** -0.5, 0.25, ((0, 32),))
    shared_gate = gaussian(key_of[7], (D_SHARED, D), D ** -0.5, 0.125)
    shared_up = gaussian(key_of[8], (D_SHARED, D), D ** -0.5, 0.125)
    shared_down = gaussian(key_of[9], (D_SHARED, D), D_SHARED ** -0.5, 0.375)
    return dict(tokens=tokens, expert_ids=expert_ids, route_weights=route_weights, cotangent=cotangent, gate_weight=gate_weight, up_weight=up_weight, down_weight=down_weight, shared_gate=shared_gate, shared_up=shared_up, shared_down=shared_down)


def gated_backward(scaled, gate_pre, up_pre):
    sigmoid_gate = jax.nn.sigmoid(gate_pre)
    gate_delta = (scaled * up_pre * sigmoid_gate * (1.0 + gate_pre * (1.0 - sigmoid_gate))).astype(jnp.bfloat16)
    up_delta = (scaled * jax.nn.silu(gate_pre)).astype(jnp.bfloat16)
    return gate_delta, up_delta


def slots_of(block_ids):
    one_hot = (block_ids[:, None] == jnp.arange(EXP_GROUP, dtype=jnp.int32)[None, :]).astype(jnp.int32)
    return (jnp.sum(jnp.cumsum(one_hot, axis=0) * one_hot, axis=1) - 1).astype(jnp.int32)


def reference(tokens, expert_ids, route_weights, cotangent, gate_weight, up_weight, down_weight, shared_gate, shared_up, shared_down):
    blocks = TOKENS // TOK_DEV
    local_ids = expert_ids.reshape(blocks, TOK_DEV * TOP).astype(jnp.int32)
    slot_index = jax.vmap(slots_of)(local_ids)
    block_index = jnp.arange(blocks, dtype=jnp.int32)[:, None]
    group_index = block_index % GROUPS
    source_index = block_index // GROUPS
    expert_index = local_ids * GROUPS + group_index
    position = ((expert_index * EXP_GROUP + source_index) * CAP + slot_index).reshape(-1).astype(jnp.int32)
    assign_count = TOKENS * TOP
    rows_each = EXP_GROUP * CAP
    slots_all = EXPERTS * rows_each
    row_assign = jnp.full((slots_all,), assign_count, jnp.int32).at[position].set(jnp.arange(assign_count, dtype=jnp.int32))
    empty_row = jnp.zeros((1, D), jnp.bfloat16)
    padded_tokens = jnp.concatenate([tokens, empty_row], axis=0)
    padded_cot = jnp.concatenate([cotangent, empty_row], axis=0)
    padded_weights = jnp.concatenate([route_weights.reshape(-1), jnp.zeros((1,), jnp.float32)], axis=0)

    def expert_step(carry, inputs):
        token_acc, route_acc = carry
        gate_w, up_w, down_w, assign = inputs
        row_ids = (assign // TOP).astype(jnp.int32)
        weights = jnp.take(padded_weights, assign, axis=0)
        token_rows = jnp.take(padded_tokens, row_ids, axis=0)
        cot_rows = jnp.take(padded_cot, row_ids, axis=0)
        gate_pre = jnp.dot(token_rows, gate_w.T, preferred_element_type=jnp.float32)
        up_pre = jnp.dot(token_rows, up_w.T, preferred_element_type=jnp.float32)
        hidden = (jax.nn.silu(gate_pre) * up_pre).astype(jnp.bfloat16)
        back_hidden = jnp.dot(cot_rows, down_w.T, preferred_element_type=jnp.float32)
        route_part = jnp.sum(back_hidden * hidden.astype(jnp.float32), axis=1)
        gate_delta, up_delta = gated_backward(weights[:, None] * back_hidden, gate_pre, up_pre)
        weighted_cot = (weights[:, None] * cot_rows.astype(jnp.float32)).astype(jnp.bfloat16)
        token_part = jnp.dot(gate_delta, gate_w, preferred_element_type=jnp.float32) + jnp.dot(up_delta, up_w, preferred_element_type=jnp.float32)
        grad_gate = jnp.dot(gate_delta.T, token_rows, preferred_element_type=jnp.float32).astype(jnp.bfloat16)
        grad_up = jnp.dot(up_delta.T, token_rows, preferred_element_type=jnp.float32).astype(jnp.bfloat16)
        grad_down = jnp.dot(hidden.T, weighted_cot, preferred_element_type=jnp.float32).astype(jnp.bfloat16)
        token_acc = token_acc.at[row_ids].add(token_part)
        route_acc = route_acc.at[assign].set(route_part)
        return (token_acc, route_acc), (grad_gate, grad_up, grad_down)

    start = (jnp.zeros((TOKENS + 1, D), jnp.float32), jnp.zeros((assign_count + 1,), jnp.float32))
    (token_acc, route_acc), (gate_grad, up_grad, down_grad) = lax.scan(
        expert_step, start, (gate_weight, up_weight, down_weight, row_assign.reshape(EXPERTS, rows_each)))
    routed = token_acc[:TOKENS]
    route_grad = route_acc[:assign_count].reshape(TOKENS, TOP)

    common_gate = jnp.dot(tokens, shared_gate.T, preferred_element_type=jnp.float32)
    common_up = jnp.dot(tokens, shared_up.T, preferred_element_type=jnp.float32)
    common_hidden = (jax.nn.silu(common_gate) * common_up).astype(jnp.bfloat16)
    common_back = jnp.dot(cotangent, shared_down.T, preferred_element_type=jnp.float32)
    common_gate_delta, common_up_delta = gated_backward(common_back, common_gate, common_up)
    common_part = jnp.dot(common_gate_delta, shared_gate, preferred_element_type=jnp.float32) + jnp.dot(common_up_delta, shared_up, preferred_element_type=jnp.float32)
    shared_grads = jnp.stack([
        jnp.dot(tokens.T, common_gate_delta, preferred_element_type=jnp.float32),
        jnp.dot(tokens.T, common_up_delta, preferred_element_type=jnp.float32),
        jnp.dot(cotangent.T, common_hidden, preferred_element_type=jnp.float32)], axis=1)
    token_grad = (routed + common_part).astype(jnp.bfloat16)
    return (token_grad, route_grad, gate_grad, up_grad, down_grad, shared_grads)
```

```python
import functools

import jax
import jax.numpy as jnp
from jax import lax
from jax.experimental import pallas as pl
from jax.experimental.pallas import tpu as pltpu
from jax.sharding import PartitionSpec as P


def gated_backward(scaled, gate_pre, up_pre):
    sigmoid_gate = jax.nn.sigmoid(gate_pre)
    gate_delta = (scaled * up_pre * sigmoid_gate * (1.0 + gate_pre * (1.0 - sigmoid_gate))).astype(
        jnp.bfloat16
    )
    up_delta = (scaled * jax.nn.silu(gate_pre)).astype(jnp.bfloat16)
    return (gate_delta, up_delta)


def forward_products(token_rows, gate_local, up_local):
    gate_pre = jnp.einsum("rd,fd->rf", token_rows, gate_local, preferred_element_type=jnp.float32)
    up_pre = jnp.einsum("rd,fd->rf", token_rows, up_local, preferred_element_type=jnp.float32)
    return (gate_pre, up_pre)


def exchanged_shards(
    tokens,
    expert_ids,
    route_weights,
    cotangent,
    gate_weight,
    up_weight,
    down_weight,
    shared_gate,
    shared_up,
    shared_down,
):
    ep_size = lax.axis_size("ep")
    tok_rows = tokens.shape[0]
    model_width = tokens.shape[1]
    top_count = expert_ids.shape[1]
    capacity = 3 * tok_rows * top_count // (2 * ep_size)
    slots_all = ep_size * capacity
    assign_count = tok_rows * top_count
    flat_ids = expert_ids.reshape(-1)
    one_hot = (flat_ids[:, None] == jnp.arange(ep_size, dtype=jnp.int32)[None, :]).astype(jnp.int32)
    slot_index = jnp.sum(jnp.cumsum(one_hot, axis=0) * one_hot, axis=1) - 1
    position = flat_ids * capacity + slot_index
    row_assign = (
        jnp.full((slots_all,), assign_count, jnp.int32)
        .at[position]
        .set(jnp.arange(assign_count, dtype=jnp.int32))
    )
    row_token = row_assign // top_count
    row_weight = jnp.take(
        jnp.concatenate([route_weights.reshape(-1), jnp.zeros((1,), jnp.float32)], axis=0),
        row_assign,
        axis=0,
    )
    empty_row = jnp.zeros((1, model_width), jnp.bfloat16)
    send_tokens = jnp.take(jnp.concatenate([tokens, empty_row], axis=0), row_token, axis=0).reshape(
        ep_size, capacity, model_width
    )
    send_cot = jnp.take(jnp.concatenate([cotangent, empty_row], axis=0), row_token, axis=0).reshape(
        ep_size, capacity, model_width
    )
    gate_local = gate_weight[0]
    up_local = up_weight[0]
    down_local = down_weight[0]
    scales = lax.all_to_all(
        row_weight.reshape(ep_size, capacity), "ep", split_axis=0, concat_axis=0, tiled=True
    ).reshape(slots_all)
    token_rows, cot_rows = (
        lax.all_to_all(send_tokens, "ep", split_axis=0, concat_axis=0, tiled=True),
        lax.all_to_all(send_cot, "ep", split_axis=0, concat_axis=0, tiled=True),
    )
    token_rows = token_rows.reshape(slots_all, model_width)
    cot_rows = cot_rows.reshape(slots_all, model_width)
    gate_pre, up_pre = forward_products(token_rows, gate_local, up_local)
    hidden = (jax.nn.silu(gate_pre) * up_pre).astype(jnp.bfloat16)
    back_hidden = jnp.einsum("rd,fd->rf", cot_rows, down_local, preferred_element_type=jnp.float32)
    route_part = jnp.sum(back_hidden * hidden.astype(jnp.float32), axis=1)
    gate_delta, up_delta = gated_backward(scales[:, None] * back_hidden, gate_pre, up_pre)
    weighted_cot = (scales[:, None] * cot_rows.astype(jnp.float32)).astype(jnp.bfloat16)
    token_part = jnp.einsum(
        "rf,fd->rd", gate_delta, gate_local, preferred_element_type=jnp.float32
    ) + jnp.einsum("rf,fd->rd", up_delta, up_local, preferred_element_type=jnp.float32)
    gate_grad = jnp.einsum(
        "rf,rd->fd", gate_delta, token_rows, preferred_element_type=jnp.float32
    ).astype(jnp.bfloat16)[None]
    up_grad = jnp.einsum(
        "rf,rd->fd", up_delta, token_rows, preferred_element_type=jnp.float32
    ).astype(jnp.bfloat16)[None]
    down_grad = jnp.einsum(
        "rf,rd->fd", hidden, weighted_cot, preferred_element_type=jnp.float32
    ).astype(jnp.bfloat16)[None]
    back_rows, back_route = (
        lax.all_to_all(
            token_part.reshape(ep_size, capacity, model_width),
            "ep",
            split_axis=0,
            concat_axis=0,
            tiled=True,
        ),
        lax.all_to_all(
            route_part.reshape(ep_size, capacity), "ep", split_axis=0, concat_axis=0, tiled=True
        ),
    )
    routed = jnp.sum(
        jnp.take(back_rows.reshape(slots_all, model_width), position, axis=0).reshape(
            tok_rows, top_count, model_width
        ),
        axis=1,
    )
    route_grad = jnp.take(back_route.reshape(slots_all), position, axis=0).reshape(
        tok_rows, top_count
    )
    common_gate = jnp.einsum("td,fd->tf", tokens, shared_gate, preferred_element_type=jnp.float32)
    common_up = jnp.einsum("td,fd->tf", tokens, shared_up, preferred_element_type=jnp.float32)
    common_hidden = (jax.nn.silu(common_gate) * common_up).astype(jnp.bfloat16)
    common_back = jnp.einsum(
        "td,fd->tf", cotangent, shared_down, preferred_element_type=jnp.float32
    )
    common_gate_delta, common_up_delta = gated_backward(common_back, common_gate, common_up)
    common_part = jnp.einsum(
        "tf,fd->td", common_gate_delta, shared_gate, preferred_element_type=jnp.float32
    ) + jnp.einsum("tf,fd->td", common_up_delta, shared_up, preferred_element_type=jnp.float32)
    shared_grads = lax.psum_scatter(
        jnp.stack(
            [
                jnp.einsum(
                    "tc,tf->cf", tokens, common_gate_delta, preferred_element_type=jnp.float32
                ),
                jnp.einsum(
                    "tc,tf->cf", tokens, common_up_delta, preferred_element_type=jnp.float32
                ),
                jnp.einsum(
                    "tc,tf->cf", cotangent, common_hidden, preferred_element_type=jnp.float32
                ),
            ],
            axis=1,
        ),
        ("ep", "tp"),
        scatter_dimension=0,
        tiled=True,
    )
    token_grad = (routed + common_part).astype(jnp.bfloat16)
    return (token_grad, route_grad, gate_grad, up_grad, down_grad, shared_grads)


MESH = pl.DeviceIdType.MESH


def ring_place(index, count):
    odd = lax.rem(index, 2)
    pair = lax.div(index, 2)
    return (1 - odd) * pair + odd * (count - 1 - pair)


def ring_index(place, count):
    place = lax.rem(place + 2 * count, count)
    late = lax.div(place, (count + 1) // 2)
    return (1 - late) * (2 * place) + late * (2 * (count - 1 - place) + 1)


def greet(groups):
    barrier = pltpu.get_barrier_semaphore()
    total = 0
    for axis, count in groups:
        me = lax.axis_index(axis)
        for step in range(1, count):
            pl.semaphore_signal(
                barrier,
                inc=1,
                device_id={axis: lax.rem(me + step, count)},
                device_id_type=MESH,
            )
            total += 1
    pl.semaphore_wait(barrier, total)


def remote(src, dst, send_sem, recv_sem, axis, index):
    return pltpu.make_async_remote_copy(
        src_ref=src,
        dst_ref=dst,
        send_sem=send_sem,
        recv_sem=recv_sem,
        device_id={axis: index},
        device_id_type=MESH,
    )


def spread_rows(src, dst, send_sem, recv_sem, axis, count):
    me = lax.axis_index(axis)
    copies = []
    for step in range(1, count):
        peer = lax.rem(me + step, count)
        copies.append(
            remote(src.at[peer], dst.at[me], send_sem.at[step - 1], recv_sem.at[step - 1], axis, peer)
        )
    return copies


def dot_nt(left, right):
    return lax.dot_general(
        left, right, (((1,), (1,)), ((), ())), preferred_element_type=jnp.float32
    )


def deltas(scaled, gate_pre, up_pre):
    sigmoid_gate = jax.nn.sigmoid(gate_pre)
    silu_gate = gate_pre * sigmoid_gate
    gate_delta = scaled * up_pre * sigmoid_gate * (1.0 + gate_pre * (1.0 - sigmoid_gate))
    return gate_delta, scaled * silu_gate, silu_gate * up_pre


def layer_kernel(
    count,
    group,
    tok,
    cot,
    ids,
    chosen_w,
    gate_w,
    up_w,
    down_w,
    shared_gate,
    shared_up,
    shared_down,
    token_out,
    route_out,
    gate_out,
    up_out,
    down_out,
    shared_out,
    wts,
    route_in,
    all_tok,
    all_cot,
    all_wts,
    tok_w,
    cot_w,
    pre,
    turned,
    shared_turned,
    part,
    own_part,
    held,
    outgoing,
    route_buf,
    shared_part,
    shared_send,
    shared_in,
    total_grad,
    gsend,
    grecv,
    rsend,
    rrecv,
    load_sem,
    wsend,
    wrecv,
    bsend,
    brecv,
    ssend,
    srecv,
    own_sem,
):
    me = lax.axis_index("ep")
    mine = lax.axis_index("tp")
    place = ring_place(me, count)
    rows, width = tok.shape
    half = rows // 2
    hid = gate_w.shape[0]
    common = shared_gate.shape[0]
    sides = (ring_index(place + 1, count), ring_index(place - 1, count))
    halves = (pl.ds(0, half), pl.ds(half, half))

    loads = [
        pltpu.make_async_copy(src, dst, load_sem.at[i])
        for i, (src, dst) in enumerate(
            (
                (tok, all_tok.at[0]),
                (cot, all_cot.at[0]),
                (gate_w, tok_w.at[pl.ds(0, hid)]),
                (up_w, tok_w.at[pl.ds(hid, hid)]),
                (shared_gate, tok_w.at[pl.ds(2 * hid, common)]),
                (shared_up, tok_w.at[pl.ds(2 * hid + common, common)]),
                (down_w, cot_w.at[pl.ds(0, hid)]),
                (shared_down, cot_w.at[pl.ds(hid, common)]),
            )
        )
    ]
    for copy in loads:
        copy.start()
    for expert in range(count):
        wts[expert] = jnp.sum(
            jnp.where(ids[...] == expert, chosen_w[...], 0.0), axis=0, keepdims=True
        )
    greet((("ep", count), ("tp", group)))

    def passed(step, array, side):
        slots = (all_tok, all_cot)[array]
        return remote(
            slots.at[step, halves[side]],
            slots.at[step + 1, halves[side]],
            gsend.at[array, side, step],
            grecv.at[array, side, step],
            "ep",
            sides[side],
        )

    def hop(step, side):
        return remote(
            outgoing.at[step - 1, halves[side]],
            held.at[step - 1, halves[side]],
            rsend.at[side, step - 1],
            rrecv.at[side, step - 1],
            "ep",
            sides[side],
        )

    loads[0].wait()
    passed(0, 0, 0).start()
    passed(0, 0, 1).start()
    loads[1].wait()
    passed(0, 1, 0).start()
    passed(0, 1, 1).start()
    weights = spread_rows(wts, all_wts, wsend, wrecv, "ep", count)
    for copy in weights:
        copy.start()
    own_weights = pltpu.make_async_copy(wts.at[me], all_wts.at[me], own_sem.at[0])
    own_weights.start()
    route_buf[...] = jnp.zeros_like(route_buf)
    for copy in loads[2:]:
        copy.wait()
    for copy in weights:
        copy.wait()
    own_weights.wait()

    outs = (gate_out, up_out, down_out)
    early = [count - 3 + i for i in range(3)]
    tile = width // count

    def add_tiles(i, start, end, last):
        slots = all_cot if i == 2 else all_tok

        def tile_body(j, carry):
            cols = pl.ds(pl.multiple_of(j * tile, tile), tile)
            block = slots[pl.ds(start, end - start), :, cols].reshape((end - start) * rows, tile)
            left = turned[i, :, pl.ds(start * rows, (end - start) * rows)]
            grad = jnp.dot(left, block, preferred_element_type=jnp.float32)
            if last:
                outs[i][:, cols] = (total_grad[i, :, cols] + grad).astype(jnp.bfloat16)
            else:
                total_grad[i, :, cols] = grad
            return carry

        lax.fori_loop(0, count, tile_body, 0)

    def body(step, carry):
        def pass_on(array):
            @pl.when(step > 0)
            def _():
                for side in (0, 1):
                    passed(step - 1, array, side).wait_recv()

                    @pl.when(step < count - 1)
                    def _():
                        passed(step, array, side).start()

        pass_on(0)
        first = ring_index(place - step, count)
        second = ring_index(place + step, count)
        lane = lax.broadcasted_iota(jnp.int32, (1, rows), 1)
        eye = lax.broadcasted_iota(jnp.int32, (rows, rows), 0) == lax.broadcasted_iota(
            jnp.int32, (rows, rows), 1
        )
        scale_row = jnp.where(lane < half, all_wts[first], all_wts[second])
        scale = jnp.sum(jnp.where(eye, scale_row, 0.0), axis=1, keepdims=True)

        pre[...] = dot_nt(all_tok[step], tok_w[...])
        pass_on(1)
        back_hidden = dot_nt(all_cot[step], cot_w[pl.ds(0, hid)])
        gate_pre, up_pre = pre[:, pl.ds(0, hid)], pre[:, pl.ds(hid, hid)]
        gate_delta, up_delta, hidden = deltas(scale * back_hidden, gate_pre, up_pre)
        both = jnp.concatenate([gate_delta, up_delta], axis=1).astype(jnp.bfloat16)
        part[...] = jnp.dot(both, tok_w[pl.ds(0, 2 * hid)], preferred_element_type=jnp.float32)

        @pl.when(step == 1)
        def _():
            outgoing[0] = part[...].astype(jnp.bfloat16)
            for side in (0, 1):
                hop(step, side).start()

        @pl.when(step > 1)
        def _():
            for side in (0, 1):
                hop(step - 1, side).wait_recv()
                outgoing[step - 1, halves[side]] = (
                    held[step - 2, halves[side]].astype(jnp.float32) + part[halves[side]]
                ).astype(jnp.bfloat16)
                hop(step, side).start()

        rounded = hidden.astype(jnp.bfloat16).astype(jnp.float32)
        route = jnp.sum(back_hidden * rounded, axis=1, keepdims=True)
        route_row = jnp.sum(jnp.where(eye, route, 0.0), axis=0, keepdims=True)
        route_buf[first] = jnp.where(lane < half, route_row, route_buf[first])
        route_buf[second] = jnp.where(lane < half, route_buf[second], route_row)
        columns = pl.ds(pl.multiple_of(step * rows, rows), rows)
        turned[0, :, columns] = gate_delta.T.astype(jnp.bfloat16)
        turned[1, :, columns] = up_delta.T.astype(jnp.bfloat16)
        turned[2, :, columns] = (scale * hidden).T.astype(jnp.bfloat16)

        common_back = dot_nt(all_cot[step], cot_w[pl.ds(hid, common)])
        common_gate = pre[:, pl.ds(2 * hid, common)]
        common_up = pre[:, pl.ds(2 * hid + common, common)]
        common_deltas = deltas(common_back, common_gate, common_up)
        for i in range(3):
            shared_turned[i, :, columns] = common_deltas[i].T.astype(jnp.bfloat16)

        @pl.when(step == 0)
        def _():
            pair = jnp.concatenate(common_deltas[:2], axis=1).astype(jnp.bfloat16)
            own_part[...] = part[...] + jnp.dot(
                pair, tok_w[pl.ds(2 * hid, 2 * common)], preferred_element_type=jnp.float32
            )

        for i in range(3):

            @pl.when(step == count - 4 + i)
            def _():
                add_tiles(i, 0, early[i], False)

        return carry

    lax.fori_loop(0, count, body, 0)

    span = width // count
    piece = span // group
    mine_cols = pl.ds(pl.multiple_of(me * span, span), span)
    for i, slots in enumerate((all_tok, all_tok, all_cot)):
        block = slots[:, :, mine_cols].reshape(count * rows, span)
        grad = jnp.dot(shared_turned[i], block, preferred_element_type=jnp.float32).T
        for peer in range(group):
            shared_part[peer, i] = grad[peer * piece : (peer + 1) * piece]
            shared_send[peer, i] = grad[peer * piece : (peer + 1) * piece].astype(jnp.bfloat16)
    small = spread_rows(route_buf, route_in, bsend, brecv, "ep", count)
    small += spread_rows(shared_send, shared_in, ssend, srecv, "tp", group)
    for copy in small:
        copy.start()
    own_route = pltpu.make_async_copy(route_buf.at[me], route_in.at[me], own_sem.at[1])
    own_route.start()

    for i in range(3):
        add_tiles(i, early[i], count, True)

    for side in (0, 1):
        hop(count - 1, side).wait_recv()
        token_out[halves[side]] = (
            held[count - 2, halves[side]].astype(jnp.float32) + own_part[halves[side]]
        ).astype(jnp.bfloat16)
    for copy in small:
        copy.wait()
    own_route.wait()
    routes = jnp.zeros(ids.shape, jnp.float32)
    for expert in range(count):
        routes = jnp.where(ids[...] == expert, route_in[expert], routes)
    route_out[...] = routes
    total = shared_part[mine]
    for step in range(1, group):
        total = total + shared_in[lax.rem(mine + step, group)].astype(jnp.float32)
    shared_out[...] = total
    for step in range(count - 1):
        for side in (0, 1):
            for array in (0, 1):
                passed(step, array, side).wait_send()
            hop(step + 1, side).wait_send()


def layer(tokens, cotangent, ids, weights, experts, commons, count, group):
    rows, width = tokens.shape
    hid, common = experts[0].shape[0], commons[0].shape[0]
    piece = width // count // group
    vmem = pl.BlockSpec(memory_space=pltpu.VMEM)
    anywhere = pl.BlockSpec(memory_space=pl.ANY)
    grad = pltpu.VMEM((hid, width), jnp.bfloat16)
    shared = (3, piece, common)
    return pl.pallas_call(
        functools.partial(layer_kernel, count, group),
        out_shape=(
            pltpu.VMEM((rows, width), jnp.bfloat16),
            pltpu.VMEM(ids.shape, jnp.float32),
            grad,
            grad,
            grad,
            pltpu.VMEM(shared, jnp.float32),
        ),
        in_specs=[anywhere, anywhere, vmem, vmem] + [anywhere] * 6,
        out_specs=(vmem,) * 6,
        scratch_shapes=[
            pltpu.VMEM((count, 1, rows), jnp.float32),
            pltpu.VMEM((count, 1, rows), jnp.float32),
            pltpu.VMEM((count, rows, width), jnp.bfloat16),
            pltpu.VMEM((count, rows, width), jnp.bfloat16),
            pltpu.VMEM((count, 1, rows), jnp.float32),
            pltpu.VMEM((2 * hid + 2 * common, width), jnp.bfloat16),
            pltpu.VMEM((hid + common, width), jnp.bfloat16),
            pltpu.VMEM((rows, 2 * hid + 2 * common), jnp.float32),
            pltpu.VMEM((3, hid, count * rows), jnp.bfloat16),
            pltpu.VMEM((3, common, count * rows), jnp.bfloat16),
            pltpu.VMEM((rows, width), jnp.float32),
            pltpu.VMEM((rows, width), jnp.float32),
            pltpu.VMEM((count - 1, rows, width), jnp.bfloat16),
            pltpu.VMEM((count - 1, rows, width), jnp.bfloat16),
            pltpu.VMEM((count, 1, rows), jnp.float32),
            pltpu.VMEM((group,) + shared, jnp.float32),
            pltpu.VMEM((group,) + shared, jnp.bfloat16),
            pltpu.VMEM((group,) + shared, jnp.bfloat16),
            pltpu.VMEM((3, hid, width), jnp.float32),
            pltpu.SemaphoreType.DMA((2, 2, count - 1)),
            pltpu.SemaphoreType.DMA((2, 2, count - 1)),
            pltpu.SemaphoreType.DMA((2, count - 1)),
            pltpu.SemaphoreType.DMA((2, count - 1)),
            pltpu.SemaphoreType.DMA((8,)),
            pltpu.SemaphoreType.DMA((count - 1,)),
            pltpu.SemaphoreType.DMA((count - 1,)),
            pltpu.SemaphoreType.DMA((count - 1,)),
            pltpu.SemaphoreType.DMA((count - 1,)),
            pltpu.SemaphoreType.DMA((group - 1,)),
            pltpu.SemaphoreType.DMA((group - 1,)),
            pltpu.SemaphoreType.DMA((2,)),
        ],
        compiler_params=pltpu.CompilerParams(
            collective_id=0, has_side_effects=True, vmem_limit_bytes=53 * 2**20
        ),
    )(tokens, cotangent, ids, weights, *experts, *commons)


def flush_kernel(count, *refs):
    copies = [
        pltpu.make_async_copy(refs[i], refs[count + i], refs[2 * count].at[i]) for i in range(count)
    ]
    for copy in copies:
        copy.start()
    for copy in copies:
        copy.wait()


def flush(*held):
    count = len(held)
    return pl.pallas_call(
        functools.partial(flush_kernel, count),
        out_shape=tuple(jax.ShapeDtypeStruct(x.shape, x.dtype) for x in held),
        in_specs=[pl.BlockSpec(memory_space=pltpu.VMEM)] * count,
        out_specs=(pl.BlockSpec(memory_space=pl.ANY),) * count,
        scratch_shapes=[pltpu.SemaphoreType.DMA((count,))],
        compiler_params=pltpu.CompilerParams(vmem_limit_bytes=2**20),
    )(*held)


def gathered_shards(
    tokens,
    expert_ids,
    route_weights,
    cotangent,
    gate_weight,
    up_weight,
    down_weight,
    shared_gate,
    shared_up,
    shared_down,
):
    count, group = lax.axis_size("ep"), lax.axis_size("tp")
    held = layer(
        tokens,
        cotangent,
        expert_ids.T,
        route_weights.T,
        (gate_weight[0], up_weight[0], down_weight[0]),
        (shared_gate, shared_up, shared_down),
        count,
        group,
    )
    token_grad, route_grad, gate_grad, up_grad, down_grad, shared_sum = flush(*held)
    return (
        token_grad,
        route_grad.T,
        gate_grad[None],
        up_grad[None],
        down_grad[None],
        jnp.transpose(shared_sum, (1, 0, 2)),
    )


def shards(tokens, expert_ids, *rest):
    dense = 4 <= lax.axis_size("ep") <= 2 * expert_ids.shape[1]
    return (gathered_shards if dense else exchanged_shards)(tokens, expert_ids, *rest)


def solution(mesh):
    in_specs = (
        P(("ep", "tp"), None),
        P(("ep", "tp"), None),
        P(("ep", "tp"), None),
        P(("ep", "tp"), None),
        P(("ep", "tp"), None, None),
        P(("ep", "tp"), None, None),
        P(("ep", "tp"), None, None),
        P(),
        P(),
        P(),
    )
    out_specs = (
        P(("ep", "tp"), None),
        P(("ep", "tp"), None),
        P(("ep", "tp"), None, None),
        P(("ep", "tp"), None, None),
        P(("ep", "tp"), None, None),
        P(("ep", "tp"), None, None),
    )
    return jax.shard_map(shards, mesh=mesh, in_specs=in_specs, out_specs=out_specs, check_vma=False)
```

```python
import functools

import jax
import jax.numpy as jnp
from jax import lax
from jax.experimental import pallas as pl
from jax.experimental.pallas import tpu as pltpu
from jax.sharding import PartitionSpec as P


def gated_backward(scaled, gate_pre, up_pre):
    sigmoid_gate = jax.nn.sigmoid(gate_pre)
    gate_delta = (scaled * up_pre * sigmoid_gate * (1.0 + gate_pre * (1.0 - sigmoid_gate))).astype(
        jnp.bfloat16
    )
    up_delta = (scaled * jax.nn.silu(gate_pre)).astype(jnp.bfloat16)
    return (gate_delta, up_delta)


def forward_products(token_rows, gate_local, up_local):
    gate_pre = jnp.einsum("rd,fd->rf", token_rows, gate_local, preferred_element_type=jnp.float32)
    up_pre = jnp.einsum("rd,fd->rf", token_rows, up_local, preferred_element_type=jnp.float32)
    return (gate_pre, up_pre)


def exchanged_shards(
    tokens,
    expert_ids,
    route_weights,
    cotangent,
    gate_weight,
    up_weight,
    down_weight,
    shared_gate,
    shared_up,
    shared_down,
):
    ep_size = lax.axis_size("ep")
    tok_rows = tokens.shape[0]
    model_width = tokens.shape[1]
    top_count = expert_ids.shape[1]
    capacity = 3 * tok_rows * top_count // (2 * ep_size)
    slots_all = ep_size * capacity
    assign_count = tok_rows * top_count
    flat_ids = expert_ids.reshape(-1)
    one_hot = (flat_ids[:, None] == jnp.arange(ep_size, dtype=jnp.int32)[None, :]).astype(jnp.int32)
    slot_index = jnp.sum(jnp.cumsum(one_hot, axis=0) * one_hot, axis=1) - 1
    position = flat_ids * capacity + slot_index
    row_assign = (
        jnp.full((slots_all,), assign_count, jnp.int32)
        .at[position]
        .set(jnp.arange(assign_count, dtype=jnp.int32))
    )
    row_token = row_assign // top_count
    row_weight = jnp.take(
        jnp.concatenate([route_weights.reshape(-1), jnp.zeros((1,), jnp.float32)], axis=0),
        row_assign,
        axis=0,
    )
    empty_row = jnp.zeros((1, model_width), jnp.bfloat16)
    send_tokens = jnp.take(jnp.concatenate([tokens, empty_row], axis=0), row_token, axis=0).reshape(
        ep_size, capacity, model_width
    )
    send_cot = jnp.take(jnp.concatenate([cotangent, empty_row], axis=0), row_token, axis=0).reshape(
        ep_size, capacity, model_width
    )
    gate_local = gate_weight[0]
    up_local = up_weight[0]
    down_local = down_weight[0]
    scales = lax.all_to_all(
        row_weight.reshape(ep_size, capacity), "ep", split_axis=0, concat_axis=0, tiled=True
    ).reshape(slots_all)
    token_rows, cot_rows = (
        lax.all_to_all(send_tokens, "ep", split_axis=0, concat_axis=0, tiled=True),
        lax.all_to_all(send_cot, "ep", split_axis=0, concat_axis=0, tiled=True),
    )
    token_rows = token_rows.reshape(slots_all, model_width)
    cot_rows = cot_rows.reshape(slots_all, model_width)
    gate_pre, up_pre = forward_products(token_rows, gate_local, up_local)
    hidden = (jax.nn.silu(gate_pre) * up_pre).astype(jnp.bfloat16)
    back_hidden = jnp.einsum("rd,fd->rf", cot_rows, down_local, preferred_element_type=jnp.float32)
    route_part = jnp.sum(back_hidden * hidden.astype(jnp.float32), axis=1)
    gate_delta, up_delta = gated_backward(scales[:, None] * back_hidden, gate_pre, up_pre)
    weighted_cot = (scales[:, None] * cot_rows.astype(jnp.float32)).astype(jnp.bfloat16)
    token_part = jnp.einsum(
        "rf,fd->rd", gate_delta, gate_local, preferred_element_type=jnp.float32
    ) + jnp.einsum("rf,fd->rd", up_delta, up_local, preferred_element_type=jnp.float32)
    gate_grad = jnp.einsum(
        "rf,rd->fd", gate_delta, token_rows, preferred_element_type=jnp.float32
    ).astype(jnp.bfloat16)[None]
    up_grad = jnp.einsum(
        "rf,rd->fd", up_delta, token_rows, preferred_element_type=jnp.float32
    ).astype(jnp.bfloat16)[None]
    down_grad = jnp.einsum(
        "rf,rd->fd", hidden, weighted_cot, preferred_element_type=jnp.float32
    ).astype(jnp.bfloat16)[None]
    back_rows, back_route = (
        lax.all_to_all(
            token_part.reshape(ep_size, capacity, model_width),
            "ep",
            split_axis=0,
            concat_axis=0,
            tiled=True,
        ),
        lax.all_to_all(
            route_part.reshape(ep_size, capacity), "ep", split_axis=0, concat_axis=0, tiled=True
        ),
    )
    routed = jnp.sum(
        jnp.take(back_rows.reshape(slots_all, model_width), position, axis=0).reshape(
            tok_rows, top_count, model_width
        ),
        axis=1,
    )
    route_grad = jnp.take(back_route.reshape(slots_all), position, axis=0).reshape(
        tok_rows, top_count
    )
    common_gate = jnp.einsum("td,fd->tf", tokens, shared_gate, preferred_element_type=jnp.float32)
    common_up = jnp.einsum("td,fd->tf", tokens, shared_up, preferred_element_type=jnp.float32)
    common_hidden = (jax.nn.silu(common_gate) * common_up).astype(jnp.bfloat16)
    common_back = jnp.einsum(
        "td,fd->tf", cotangent, shared_down, preferred_element_type=jnp.float32
    )
    common_gate_delta, common_up_delta = gated_backward(common_back, common_gate, common_up)
    common_part = jnp.einsum(
        "tf,fd->td", common_gate_delta, shared_gate, preferred_element_type=jnp.float32
    ) + jnp.einsum("tf,fd->td", common_up_delta, shared_up, preferred_element_type=jnp.float32)
    shared_grads = lax.psum_scatter(
        jnp.stack(
            [
                jnp.einsum(
                    "tc,tf->cf", tokens, common_gate_delta, preferred_element_type=jnp.float32
                ),
                jnp.einsum(
                    "tc,tf->cf", tokens, common_up_delta, preferred_element_type=jnp.float32
                ),
                jnp.einsum(
                    "tc,tf->cf", cotangent, common_hidden, preferred_element_type=jnp.float32
                ),
            ],
            axis=1,
        ),
        ("ep", "tp"),
        scatter_dimension=0,
        tiled=True,
    )
    token_grad = (routed + common_part).astype(jnp.bfloat16)
    return (token_grad, route_grad, gate_grad, up_grad, down_grad, shared_grads)


MESH = pl.DeviceIdType.MESH
LEVELS = 4
PIECES = 4


def greet(peers):
    barrier = pltpu.get_barrier_semaphore()
    for peer in peers:
        pl.semaphore_signal(barrier, inc=1, device_id=peer, device_id_type=MESH)
    pl.semaphore_wait(barrier, len(peers))


def remote(src, dst, send_sem, recv_sem, device):
    return pltpu.make_async_remote_copy(
        src_ref=src,
        dst_ref=dst,
        send_sem=send_sem,
        recv_sem=recv_sem,
        device_id=device,
        device_id_type=MESH,
    )


def dot_nt(left, right):
    return lax.dot_general(
        left, right, (((1,), (1,)), ((), ())), preferred_element_type=jnp.float32
    )


def dot(left, right):
    return jnp.dot(left, right, preferred_element_type=jnp.float32)


def deltas(scaled, gate_pre, up_pre):
    sigmoid_gate = jax.nn.sigmoid(gate_pre)
    silu_gate = gate_pre * sigmoid_gate
    gate_delta = scaled * up_pre * sigmoid_gate * (1.0 + gate_pre * (1.0 - sigmoid_gate))
    return gate_delta, scaled * silu_gate, silu_gate * up_pre


def layer_kernel(
    count,
    group,
    cap,
    tok,
    cot,
    ids,
    chosen_w,
    gate_w,
    up_w,
    down_w,
    shared_gate,
    shared_up,
    shared_down,
    token_out,
    route_out,
    gate_out,
    up_out,
    down_out,
    shared_out,
    meta,
    all_meta,
    route_buf,
    route_in,
    tok_w,
    cot_w,
    col,
    cmp_send,
    cmp_in,
    pre,
    turned,
    shared_turned,
    own_sum,
    other_sum,
    sum_send,
    sum_in,
    other_send,
    other_in,
    cross_send,
    cross_in,
    back_send,
    back_in,
    shared_part,
    shared_send,
    shared_in,
    load_sem,
    msend,
    mrecv,
    rsend,
    rrecv,
    zsend,
    zrecv,
    xsend,
    xrecv,
    dsend,
    drecv,
    osend,
    orecv,
    qsend,
    qrecv,
    bsend,
    brecv,
    ssend,
    srecv,
    own_sem,
):
    me = lax.axis_index("ep")
    mine = lax.axis_index("tp")
    level, side = lax.div(me, 2), lax.rem(me, 2)
    low = 1 - lax.div(level, LEVELS // 2)
    role = low * level + (1 - low) * (LEVELS - 1 - level)
    is_end, is_mid = role == 0, role == 1
    inner = {"ep": me + 4 * low - 2}
    outer = {"ep": me - 4 * low + 2}
    partner = {"ep": me + 1 - 2 * side}
    rows, width = tok.shape
    hid = gate_w.shape[0]
    common = shared_gate.shape[0]
    cut = width // PIECES
    every = tuple(range(PIECES))
    first, second = every[: PIECES // 2], every[PIECES // 2 :]

    def block_of(lev, column):
        return 2 * (low * lev + (1 - low) * (LEVELS - 1 - lev)) + column

    def piece(h):
        return pl.ds(h * cut, cut)

    loads = [
        pltpu.make_async_copy(src, dst, load_sem.at[i])
        for i, (src, dst) in enumerate(
            (
                (tok, col.at[0, role]),
                (cot, col.at[1, role]),
                (gate_w, tok_w.at[pl.ds(0, hid)]),
                (up_w, tok_w.at[pl.ds(hid, hid)]),
                (shared_gate, tok_w.at[pl.ds(2 * hid, common)]),
                (shared_up, tok_w.at[pl.ds(2 * hid + common, common)]),
                (down_w, cot_w.at[pl.ds(0, hid)]),
                (shared_down, cot_w.at[pl.ds(hid, common)]),
            )
        )
    ]
    for copy in loads:
        copy.start()

    lane = lax.broadcasted_iota(jnp.int32, (rows, rows), 1)
    depth = lax.broadcasted_iota(jnp.int32, (rows, rows), 0)
    before = jnp.where(depth <= lane, 1.0, 0.0).astype(jnp.bfloat16)
    for expert in range(count):
        named = ids[...] == expert
        meta[expert, 0] = jnp.sum(jnp.where(named, chosen_w[...], 0.0), axis=0, keepdims=True)
        hit = jnp.sum(jnp.where(named, 1.0, 0.0), axis=0, keepdims=True)
        place = dot(jnp.broadcast_to(hit, (8, rows)).astype(jnp.bfloat16), before)[:1]
        meta[expert, 1] = jnp.where(hit > 0.0, place - 1.0, -1.0)

    peers = [{"ep": lax.rem(me + step, count)} for step in range(1, count)]
    near = []
    for turn in range(2):
        for step in range(group):
            if turn + step > 0:
                near.append((turn, step, lax.rem(side + turn, 2), lax.rem(mine + step, group)))
    greet(
        peers
        + [
            {"ep": 2 * level + to_side, "tp": to_group}
            for turn, step, to_side, to_group in near
            if step > 0
        ]
    )

    def passed(array, lev, h, inward):
        if inward:
            lands = is_end * lev + is_mid * (LEVELS - 1 - lev)
        else:
            lands = lev
        return remote(
            col.at[array, lev, :, piece(h)],
            col.at[array, lands, :, piece(h)],
            zsend.at[1 - inward, array, lev, h],
            zrecv.at[array, lands, h],
            inner if inward else outer,
        )

    def arrival(array, lev, h):
        here = col.at[array, lev, :, piece(h)]
        return remote(here, here, zsend.at[0, array, lev, h], zrecv.at[array, lev, h], inner)

    def crossed(array, lev, h):
        return remote(
            cmp_send.at[array, lev, :, piece(h)],
            cmp_in.at[array, lev, pl.ds(0, cap), piece(h)],
            xsend.at[array, lev, h],
            xrecv.at[array, lev, h],
            partner,
        )

    def summed(lev, h):
        inward = lev > 0
        lands = is_end * lev + is_mid * (LEVELS - 1 - lev) if inward else lev
        return remote(
            sum_send.at[lev, :, piece(h)],
            sum_in.at[role, lands, :, piece(h)],
            dsend.at[lev, h],
            drecv.at[role, lands, h],
            inner if inward else outer,
        )

    def sum_wait(source, lev, h):
        remote(
            sum_send.at[lev, :, piece(h)],
            sum_in.at[source, lev, :, piece(h)],
            dsend.at[lev, h],
            drecv.at[source, lev, h],
            inner,
        ).wait_recv()

    def othered(lev, h):
        inward = lev > 0
        lands = is_end * lev + is_mid * (LEVELS - 1 - lev) if inward else lev
        return remote(
            other_send.at[lev, :, piece(h)],
            other_in.at[lands, :, piece(h)],
            osend.at[lev, h],
            orecv.at[lands, h],
            inner if inward else outer,
        )

    def other_wait(lev, h):
        remote(
            other_send.at[lev, :, piece(h)],
            other_in.at[lev, :, piece(h)],
            osend.at[lev, h],
            orecv.at[lev, h],
            inner,
        ).wait_recv()

    def over(h):
        return remote(
            cross_send.at[:, piece(h)],
            cross_in.at[:, piece(h)],
            qsend.at[h],
            qrecv.at[h],
            partner,
        )

    def returned(h):
        return remote(
            back_send.at[:, piece(h)],
            back_in.at[pl.ds(0, cap), piece(h)],
            bsend.at[h],
            brecv.at[h],
            partner,
        )

    def column_of(row):
        return jnp.sum(jnp.where(depth == lane, row, 0.0), axis=1, keepdims=True)

    def picks(row):
        return depth.astype(jnp.float32) == row

    def send_compact(array, lev, pieces):
        row = all_meta[block_of(lev, side), 1 - side, 1]
        chosen = jnp.where(picks(row), 1.0, 0.0).astype(jnp.bfloat16)[:cap]
        for h in pieces:
            cmp_send[array, lev, :, piece(h)] = dot(chosen, col[array, lev, :, piece(h)]).astype(
                jnp.bfloat16
            )
            crossed(array, lev, h).start()

    def arrive(array, lev, pieces):
        for h in pieces:
            arrival(array, lev, h).wait_recv()
            if isinstance(lev, int):
                if lev == 0:
                    passed(array, lev, h, 1).start()
                else:

                    @pl.when(is_mid)
                    def _():
                        passed(array, lev, h, 0).start()

            else:

                @pl.when(is_mid)
                def _():
                    passed(array, 0, h, 1).start()

            send_compact(array, lev, (h,))

    def send_sum(lev, pieces, source):
        for h in pieces:
            total = own_sum[lev, :, piece(h)]
            if lev == 2:
                row = all_meta[block_of(lev, side), 1 - side, 1]
                spread = jnp.where(
                    lane.astype(jnp.float32) == column_of(row), 1.0, 0.0
                ).astype(jnp.bfloat16)
                returned(h).wait_recv()
                total = total + dot(spread, back_in[:, piece(h)])
            if source is not None:
                sum_wait(source, lev, h)
                total = total + sum_in[source, lev, :, piece(h)].astype(jnp.float32)
            sum_send[lev, :, piece(h)] = total.astype(jnp.bfloat16)
            summed(lev, h).start()

    def send_other(lev, pieces, add):
        for h in pieces:
            total = other_sum[lev, :, piece(h)]
            if add:
                other_wait(lev, h)
                total = total + other_in[lev, :, piece(h)].astype(jnp.float32)
            other_send[lev, :, piece(h)] = total.astype(jnp.bfloat16)
            othered(lev, h).start()

    def send_over(pieces):
        for h in pieces:
            other_wait(role, h)
            total = other_sum[role, :, piece(h)] + other_in[role, :, piece(h)].astype(jnp.float32)
            cross_send[:, piece(h)] = total.astype(jnp.bfloat16)
            over(h).start()

    loads[0].wait()
    for h in every:
        passed(0, role, h, 1).start()

    @pl.when(is_mid)
    def _():
        for h in every:
            passed(0, 1, h, 0).start()

    loads[1].wait()

    @pl.when(is_end)
    def _():
        for h in every:
            passed(1, 0, h, 1).start()

    @pl.when(is_mid)
    def _():
        for h in every:
            passed(1, 1, h, 0).start()

    metas = []
    for step in range(1, count):
        peer = lax.rem(me + step, count)
        metas.append(
            remote(
                meta.at[pl.ds(2 * lax.div(peer, 2), 2)],
                all_meta.at[me],
                msend.at[step - 1],
                mrecv.at[step - 1],
                {"ep": peer},
            )
        )
    for copy in metas:
        copy.start()
    all_meta[me] = meta[pl.ds(2 * level, 2)]
    for array in (0, 1):
        send_compact(array, role, every)
    cmp_in[:, :, cap:] = jnp.zeros((2, LEVELS, rows - cap, width), jnp.bfloat16)
    back_in[cap:] = jnp.zeros((rows - cap, width), jnp.bfloat16)
    for copy in loads[2:]:
        copy.wait()
    for copy in metas:
        copy.wait()

    def full(lev, head):
        block = block_of(lev, side)
        same = depth == lane
        scale = column_of(all_meta[block, side, 0])
        pre[...] = dot_nt(col[0, lev], tok_w[...])
        back_hidden = dot_nt(col[1, lev], cot_w[pl.ds(0, hid)])
        gate_pre, up_pre = pre[:, pl.ds(0, hid)], pre[:, pl.ds(hid, hid)]
        gate_delta, up_delta, hidden = deltas(scale * back_hidden, gate_pre, up_pre)
        both = jnp.concatenate([gate_delta, up_delta], axis=1).astype(jnp.bfloat16)
        own_sum[lev] = dot(both, tok_w[pl.ds(0, 2 * hid)])
        rounded = hidden.astype(jnp.bfloat16).astype(jnp.float32)
        route = jnp.sum(back_hidden * rounded, axis=1, keepdims=True)
        route_buf[block] = jnp.sum(jnp.where(same, route, 0.0), axis=0, keepdims=True)
        columns = pl.ds(pl.multiple_of(lev * rows, rows), rows)
        turned[0, :, columns] = gate_delta.T.astype(jnp.bfloat16)
        turned[1, :, columns] = up_delta.T.astype(jnp.bfloat16)
        turned[2, :, columns] = (scale * hidden).T.astype(jnp.bfloat16)
        common_back = dot_nt(col[1, lev], cot_w[pl.ds(hid, common)])
        common_gate = pre[:, pl.ds(2 * hid, common)]
        common_up = pre[:, pl.ds(2 * hid + common, common)]
        common_deltas = deltas(common_back, common_gate, common_up)
        for i in range(3):
            shared_turned[i, :, columns] = common_deltas[i].T.astype(jnp.bfloat16)

        @pl.when(head)
        def _():
            pair = jnp.concatenate(common_deltas[:2], axis=1).astype(jnp.bfloat16)
            own_sum[lev] = own_sum[lev] + dot(pair, tok_w[pl.ds(2 * hid, 2 * common)])

    def compact(lev, last):
        for array in (0, 1):
            for h in every:
                crossed(array, lev, h).wait_recv()
        block = block_of(lev, 1 - side)
        weight_row, row = all_meta[block, side, 0], all_meta[block, side, 1]
        chosen = picks(row)
        scale = jnp.sum(jnp.where(chosen, weight_row, 0.0), axis=1, keepdims=True)
        pre[:, pl.ds(0, 2 * hid)] = dot_nt(cmp_in[0, lev], tok_w[pl.ds(0, 2 * hid)])
        back_hidden = dot_nt(cmp_in[1, lev], cot_w[pl.ds(0, hid)])
        gate_pre, up_pre = pre[:, pl.ds(0, hid)], pre[:, pl.ds(hid, hid)]
        gate_delta, up_delta, hidden = deltas(scale * back_hidden, gate_pre, up_pre)
        both = jnp.concatenate([gate_delta, up_delta], axis=1).astype(jnp.bfloat16)
        target = jnp.where(last, depth.astype(jnp.float32)[:, :1], column_of(row))
        spread = jnp.where(lane.astype(jnp.float32) == target, 1.0, 0.0).astype(jnp.bfloat16)
        other_sum[lev] = dot(
            dot(spread, both).astype(jnp.bfloat16), tok_w[pl.ds(0, 2 * hid)]
        )
        rounded = hidden.astype(jnp.bfloat16).astype(jnp.float32)
        route = jnp.sum(back_hidden * rounded, axis=1, keepdims=True)
        route_buf[block] = jnp.sum(jnp.where(chosen, route, 0.0), axis=0, keepdims=True)
        columns = pl.ds(pl.multiple_of((LEVELS + lev) * rows, rows), rows)
        turned[0, :, columns] = gate_delta.T.astype(jnp.bfloat16)
        turned[1, :, columns] = up_delta.T.astype(jnp.bfloat16)
        turned[2, :, columns] = (scale * hidden).T.astype(jnp.bfloat16)

    def body(i, carry):
        late = lax.div(i, 2)
        lev = (1 - late) * (i + role - 2 * i * role) + late * (5 - i)
        other_near = 1 - role

        @pl.when(i == 1)
        def _():
            arrive(1, other_near, second)

            @pl.when(is_mid)
            def _():
                for h in every:
                    passed(1, 1, h, 1).start()
                arrive(0, 3, second)

        @pl.when((i == 2) & is_end)
        def _():
            send_other(1, every, False)
            arrive(1, 3, every)

        @pl.when((i == 2) & is_mid)
        def _():
            arrive(1, 2, first)

        @pl.when((i == 3) & is_end)
        def _():
            send_other(3, every, False)
            arrive(0, 2, second)
            arrive(1, 2, every)

        @pl.when((i == 3) & is_mid)
        def _():
            send_over(second)

        full(lev, i == 0)

        @pl.when(i == 0)
        def _():
            arrive(0, other_near, every)
            arrive(1, other_near, first)

            @pl.when(is_mid)
            def _():
                arrive(0, 3, first)

        @pl.when((i == 1) & is_end)
        def _():
            send_sum(1, every, None)
            arrive(0, 3, every)

        @pl.when((i == 1) & is_mid)
        def _():
            arrive(1, 3, every)
            arrive(0, 2, every)

        @pl.when((i == 2) & is_end)
        def _():
            send_sum(3, every, None)
            arrive(0, 2, first)

        @pl.when((i == 2) & is_mid)
        def _():
            arrive(1, 2, second)
            send_over(first)

        @pl.when((i == 3) & is_mid)
        def _():
            send_sum(3, every, 0)
            send_sum(0, first, 1)
            send_other(3, first, True)

        compact(lev, i == LEVELS - 1)
        return carry

    lax.fori_loop(0, LEVELS, body, 0)

    for h in every:
        back_send[:, piece(h)] = other_sum[2, pl.ds(0, cap), piece(h)].astype(jnp.bfloat16)
        returned(h).start()

    @pl.when(is_mid)
    def _():
        send_sum(0, second, 1)
        send_other(3, second, True)

    routes = []
    for step in range(1, count):
        peer = lax.rem(me + step, count)
        routes.append(
            remote(
                route_buf.at[peer],
                route_in.at[me],
                rsend.at[step - 1],
                rrecv.at[step - 1],
                {"ep": peer},
            )
        )
    for copy in routes:
        copy.start()
    route_in[me] = route_buf[me]

    tile = 2 * common
    outs = (gate_out, up_out, down_out)

    def weight_grad(i):
        array = i // 2

        def tile_body(j, carry):
            cols = pl.ds(pl.multiple_of(j * tile, tile), tile)
            reach = LEVELS * rows
            grad = dot(turned[i, :, pl.ds(0, reach)], col[array, :, :, cols].reshape(reach, tile))
            grad = grad + dot(
                turned[i, :, pl.ds(reach, reach)], cmp_in[array, :, :, cols].reshape(reach, tile)
            )
            outs[i][:, cols] = grad.astype(jnp.bfloat16)
            return carry

        lax.fori_loop(0, width // tile, tile_body, 0)

    span = width // LEVELS
    size = span // (2 * group)
    mine_cols = pl.ds(pl.multiple_of(level * span, span), span)
    for i in range(3):
        block = col[i // 2, :, :, mine_cols].reshape(LEVELS * rows, span)
        grad = dot(shared_turned[i], block).T
        for to_side in range(2):
            for to_group in range(group):
                at = (to_side * group + to_group) * size
                shared_part[to_side, to_group, i] = grad[at : at + size]
                shared_send[to_side, to_group, i] = grad[at : at + size].astype(jnp.bfloat16)
    shares = [
        remote(
            shared_send.at[to_side, to_group],
            shared_in.at[side, mine],
            ssend.at[turn, step],
            srecv.at[turn, step],
            {"ep": 2 * level + to_side, "tp": to_group},
        )
        for turn, step, to_side, to_group in near
    ]
    for copy in shares:
        copy.start()

    weight_grad(0)

    @pl.when(is_end)
    def _():
        send_sum(2, every, None)

    @pl.when(is_mid)
    def _():
        send_other(0, every, True)

    weight_grad(1)

    @pl.when(is_mid)
    def _():
        send_sum(2, every, 0)

    weight_grad(2)

    @pl.when(is_end)
    def _():
        send_over(every)

    for copy in routes:
        copy.wait()
    found = jnp.zeros(ids.shape, jnp.float32)
    for expert in range(count):
        found = jnp.where(ids[...] == expert, route_in[expert], found)
    route_out[...] = found
    for copy in shares:
        copy.wait()
    total = shared_part[side, mine]
    for turn, step, to_side, to_group in near:
        total = total + shared_in[to_side, to_group].astype(jnp.float32)
    shared_out[...] = total

    @pl.when(is_mid)
    def _():
        for h in every:
            sum_wait(0, 1, h)
            own_sum[1, :, piece(h)] = own_sum[1, :, piece(h)] + sum_in[0, 1, :, piece(h)].astype(
                jnp.float32
            )

    for h in every:
        sum_wait(1, role, h)
        total = own_sum[role, :, piece(h)] + sum_in[1, role, :, piece(h)].astype(jnp.float32)
        over(h).wait_recv()
        total = total + cross_in[:, piece(h)].astype(jnp.float32)
        token_out[:, piece(h)] = total.astype(jnp.bfloat16)

    def sent(*copies):
        for copy in copies:
            copy.wait_send()

    for h in every:
        sent(over(h), returned(h))
        for array in (0, 1):
            sent(passed(array, role, h, 1))
            for lev in range(LEVELS):
                sent(crossed(array, lev, h))

        @pl.when(is_end)
        def _():
            sent(summed(1, h), summed(2, h), summed(3, h), othered(1, h), othered(3, h))

        @pl.when(is_mid)
        def _():
            sent(summed(0, h), summed(2, h), summed(3, h), othered(0, h), othered(3, h))
            for array in (0, 1):
                sent(passed(array, 0, h, 1))
                for lev in (1, 2, 3):
                    sent(passed(array, lev, h, 0))


def layer(tokens, cotangent, ids, weights, experts, commons, count, group, cap):
    rows, width = tokens.shape
    hid, common = experts[0].shape[0], commons[0].shape[0]
    piece = width // count // group
    vmem = pl.BlockSpec(memory_space=pltpu.VMEM)
    anywhere = pl.BlockSpec(memory_space=pl.ANY)
    grad = pltpu.VMEM((hid, width), jnp.bfloat16)
    shared = (3, piece, common)
    bf16, f32, dma = jnp.bfloat16, jnp.float32, pltpu.SemaphoreType.DMA
    return pl.pallas_call(
        functools.partial(layer_kernel, count, group, cap),
        out_shape=(
            pltpu.VMEM((rows, width), bf16),
            pltpu.VMEM(ids.shape, f32),
            grad,
            grad,
            grad,
            pltpu.VMEM(shared, f32),
        ),
        in_specs=[anywhere, anywhere, vmem, vmem] + [anywhere] * 6,
        out_specs=(vmem,) * 6,
        scratch_shapes=[
            pltpu.VMEM((count, 2, 1, rows), f32),
            pltpu.VMEM((count, 2, 2, 1, rows), f32),
            pltpu.VMEM((count, 1, rows), f32),
            pltpu.VMEM((count, 1, rows), f32),
            pltpu.VMEM((2 * hid + 2 * common, width), bf16),
            pltpu.VMEM((hid + common, width), bf16),
            pltpu.VMEM((2, LEVELS, rows, width), bf16),
            pltpu.VMEM((2, LEVELS, cap, width), bf16),
            pltpu.VMEM((2, LEVELS, rows, width), bf16),
            pltpu.VMEM((rows, 2 * hid + 2 * common), f32),
            pltpu.VMEM((3, hid, 2 * LEVELS * rows), bf16),
            pltpu.VMEM((3, common, LEVELS * rows), bf16),
            pltpu.VMEM((LEVELS, rows, width), f32),
            pltpu.VMEM((LEVELS, rows, width), f32),
            pltpu.VMEM((LEVELS, rows, width), bf16),
            pltpu.VMEM((2, LEVELS, rows, width), bf16),
            pltpu.VMEM((LEVELS, rows, width), bf16),
            pltpu.VMEM((LEVELS, rows, width), bf16),
            pltpu.VMEM((rows, width), bf16),
            pltpu.VMEM((rows, width), bf16),
            pltpu.VMEM((cap, width), bf16),
            pltpu.VMEM((rows, width), bf16),
            pltpu.VMEM((2, group) + shared, f32),
            pltpu.VMEM((2, group) + shared, bf16),
            pltpu.VMEM((2, group) + shared, bf16),
            dma((8,)),
            dma((count - 1,)),
            dma((count - 1,)),
            dma((count - 1,)),
            dma((count - 1,)),
            dma((2, 2, LEVELS, PIECES)),
            dma((2, LEVELS, PIECES)),
            dma((2, LEVELS, PIECES)),
            dma((2, LEVELS, PIECES)),
            dma((LEVELS, PIECES)),
            dma((2, LEVELS, PIECES)),
            dma((LEVELS, PIECES)),
            dma((LEVELS, PIECES)),
            dma((PIECES,)),
            dma((PIECES,)),
            dma((PIECES,)),
            dma((PIECES,)),
            dma((2, group)),
            dma((2, group)),
            dma((2,)),
        ],
        compiler_params=pltpu.CompilerParams(
            collective_id=0, has_side_effects=True, vmem_limit_bytes=55 * 2**20
        ),
    )(tokens, cotangent, ids, weights, *experts, *commons)


def flush_kernel(count, *refs):
    copies = [
        pltpu.make_async_copy(refs[i], refs[count + i], refs[2 * count].at[i]) for i in range(count)
    ]
    for copy in copies:
        copy.start()
    for copy in copies:
        copy.wait()


def flush(*held):
    count = len(held)
    return pl.pallas_call(
        functools.partial(flush_kernel, count),
        out_shape=tuple(jax.ShapeDtypeStruct(x.shape, x.dtype) for x in held),
        in_specs=[pl.BlockSpec(memory_space=pltpu.VMEM)] * count,
        out_specs=(pl.BlockSpec(memory_space=pl.ANY),) * count,
        scratch_shapes=[pltpu.SemaphoreType.DMA((count,))],
        compiler_params=pltpu.CompilerParams(vmem_limit_bytes=2**20),
    )(*held)


def gathered_shards(
    tokens,
    expert_ids,
    route_weights,
    cotangent,
    gate_weight,
    up_weight,
    down_weight,
    shared_gate,
    shared_up,
    shared_down,
):
    count, group = lax.axis_size("ep"), lax.axis_size("tp")
    held = layer(
        tokens,
        cotangent,
        expert_ids.T,
        route_weights.T,
        (gate_weight[0], up_weight[0], down_weight[0]),
        (shared_gate, shared_up, shared_down),
        count,
        group,
        3 * tokens.shape[0] * expert_ids.shape[1] // (2 * count),
    )
    token_grad, route_grad, gate_grad, up_grad, down_grad, shared_sum = flush(*held)
    return (
        token_grad,
        route_grad.T,
        gate_grad[None],
        up_grad[None],
        down_grad[None],
        jnp.transpose(shared_sum, (1, 0, 2)),
    )


def shards(tokens, expert_ids, *rest):
    dense = 2 * LEVELS == lax.axis_size("ep") <= 2 * expert_ids.shape[1]
    return (gathered_shards if dense else exchanged_shards)(tokens, expert_ids, *rest)


def solution(mesh):
    in_specs = (
        P(("ep", "tp"), None),
        P(("ep", "tp"), None),
        P(("ep", "tp"), None),
        P(("ep", "tp"), None),
        P(("ep", "tp"), None, None),
        P(("ep", "tp"), None, None),
        P(("ep", "tp"), None, None),
        P(),
        P(),
        P(),
    )
    out_specs = (
        P(("ep", "tp"), None),
        P(("ep", "tp"), None),
        P(("ep", "tp"), None, None),
        P(("ep", "tp"), None, None),
        P(("ep", "tp"), None, None),
        P(("ep", "tp"), None, None),
    )
    return jax.shard_map(shards, mesh=mesh, in_specs=in_specs, out_specs=out_specs, check_vma=False)
```

```python
import functools

import jax
import jax.numpy as jnp
from jax import lax
from jax.experimental import pallas as pl
from jax.experimental.pallas import tpu as pltpu
from jax.sharding import PartitionSpec as P


def gated_backward(scaled, gate_pre, up_pre):
    sigmoid_gate = jax.nn.sigmoid(gate_pre)
    gate_delta = (scaled * up_pre * sigmoid_gate * (1.0 + gate_pre * (1.0 - sigmoid_gate))).astype(
        jnp.bfloat16
    )
    up_delta = (scaled * jax.nn.silu(gate_pre)).astype(jnp.bfloat16)
    return (gate_delta, up_delta)


def forward_products(token_rows, gate_local, up_local):
    gate_pre = jnp.einsum("rd,fd->rf", token_rows, gate_local, preferred_element_type=jnp.float32)
    up_pre = jnp.einsum("rd,fd->rf", token_rows, up_local, preferred_element_type=jnp.float32)
    return (gate_pre, up_pre)


def exchanged_shards(
    tokens,
    expert_ids,
    route_weights,
    cotangent,
    gate_weight,
    up_weight,
    down_weight,
    shared_gate,
    shared_up,
    shared_down,
):
    ep_size = lax.axis_size("ep")
    tok_rows = tokens.shape[0]
    model_width = tokens.shape[1]
    top_count = expert_ids.shape[1]
    capacity = 3 * tok_rows * top_count // (2 * ep_size)
    slots_all = ep_size * capacity
    assign_count = tok_rows * top_count
    flat_ids = expert_ids.reshape(-1)
    one_hot = (flat_ids[:, None] == jnp.arange(ep_size, dtype=jnp.int32)[None, :]).astype(jnp.int32)
    slot_index = jnp.sum(jnp.cumsum(one_hot, axis=0) * one_hot, axis=1) - 1
    position = flat_ids * capacity + slot_index
    row_assign = (
        jnp.full((slots_all,), assign_count, jnp.int32)
        .at[position]
        .set(jnp.arange(assign_count, dtype=jnp.int32))
    )
    row_token = row_assign // top_count
    row_weight = jnp.take(
        jnp.concatenate([route_weights.reshape(-1), jnp.zeros((1,), jnp.float32)], axis=0),
        row_assign,
        axis=0,
    )
    empty_row = jnp.zeros((1, model_width), jnp.bfloat16)
    send_tokens = jnp.take(jnp.concatenate([tokens, empty_row], axis=0), row_token, axis=0).reshape(
        ep_size, capacity, model_width
    )
    send_cot = jnp.take(jnp.concatenate([cotangent, empty_row], axis=0), row_token, axis=0).reshape(
        ep_size, capacity, model_width
    )
    gate_local = gate_weight[0]
    up_local = up_weight[0]
    down_local = down_weight[0]
    scales = lax.all_to_all(
        row_weight.reshape(ep_size, capacity), "ep", split_axis=0, concat_axis=0, tiled=True
    ).reshape(slots_all)
    token_rows, cot_rows = (
        lax.all_to_all(send_tokens, "ep", split_axis=0, concat_axis=0, tiled=True),
        lax.all_to_all(send_cot, "ep", split_axis=0, concat_axis=0, tiled=True),
    )
    token_rows = token_rows.reshape(slots_all, model_width)
    cot_rows = cot_rows.reshape(slots_all, model_width)
    gate_pre, up_pre = forward_products(token_rows, gate_local, up_local)
    hidden = (jax.nn.silu(gate_pre) * up_pre).astype(jnp.bfloat16)
    back_hidden = jnp.einsum("rd,fd->rf", cot_rows, down_local, preferred_element_type=jnp.float32)
    route_part = jnp.sum(back_hidden * hidden.astype(jnp.float32), axis=1)
    gate_delta, up_delta = gated_backward(scales[:, None] * back_hidden, gate_pre, up_pre)
    weighted_cot = (scales[:, None] * cot_rows.astype(jnp.float32)).astype(jnp.bfloat16)
    token_part = jnp.einsum(
        "rf,fd->rd", gate_delta, gate_local, preferred_element_type=jnp.float32
    ) + jnp.einsum("rf,fd->rd", up_delta, up_local, preferred_element_type=jnp.float32)
    gate_grad = jnp.einsum(
        "rf,rd->fd", gate_delta, token_rows, preferred_element_type=jnp.float32
    ).astype(jnp.bfloat16)[None]
    up_grad = jnp.einsum(
        "rf,rd->fd", up_delta, token_rows, preferred_element_type=jnp.float32
    ).astype(jnp.bfloat16)[None]
    down_grad = jnp.einsum(
        "rf,rd->fd", hidden, weighted_cot, preferred_element_type=jnp.float32
    ).astype(jnp.bfloat16)[None]
    back_rows, back_route = (
        lax.all_to_all(
            token_part.reshape(ep_size, capacity, model_width),
            "ep",
            split_axis=0,
            concat_axis=0,
            tiled=True,
        ),
        lax.all_to_all(
            route_part.reshape(ep_size, capacity), "ep", split_axis=0, concat_axis=0, tiled=True
        ),
    )
    routed = jnp.sum(
        jnp.take(back_rows.reshape(slots_all, model_width), position, axis=0).reshape(
            tok_rows, top_count, model_width
        ),
        axis=1,
    )
    route_grad = jnp.take(back_route.reshape(slots_all), position, axis=0).reshape(
        tok_rows, top_count
    )
    common_gate = jnp.einsum("td,fd->tf", tokens, shared_gate, preferred_element_type=jnp.float32)
    common_up = jnp.einsum("td,fd->tf", tokens, shared_up, preferred_element_type=jnp.float32)
    common_hidden = (jax.nn.silu(common_gate) * common_up).astype(jnp.bfloat16)
    common_back = jnp.einsum(
        "td,fd->tf", cotangent, shared_down, preferred_element_type=jnp.float32
    )
    common_gate_delta, common_up_delta = gated_backward(common_back, common_gate, common_up)
    common_part = jnp.einsum(
        "tf,fd->td", common_gate_delta, shared_gate, preferred_element_type=jnp.float32
    ) + jnp.einsum("tf,fd->td", common_up_delta, shared_up, preferred_element_type=jnp.float32)
    shared_grads = lax.psum_scatter(
        jnp.stack(
            [
                jnp.einsum(
                    "tc,tf->cf", tokens, common_gate_delta, preferred_element_type=jnp.float32
                ),
                jnp.einsum(
                    "tc,tf->cf", tokens, common_up_delta, preferred_element_type=jnp.float32
                ),
                jnp.einsum(
                    "tc,tf->cf", cotangent, common_hidden, preferred_element_type=jnp.float32
                ),
            ],
            axis=1,
        ),
        ("ep", "tp"),
        scatter_dimension=0,
        tiled=True,
    )
    token_grad = (routed + common_part).astype(jnp.bfloat16)
    return (token_grad, route_grad, gate_grad, up_grad, down_grad, shared_grads)


MESH = pl.DeviceIdType.MESH
LEVELS = 4
PIECES = 4


def greet(peers):
    barrier = pltpu.get_barrier_semaphore()
    for peer in peers:
        pl.semaphore_signal(barrier, inc=1, device_id=peer, device_id_type=MESH)
    return lambda: pl.semaphore_wait(barrier, len(peers))


def remote(src, dst, send_sem, recv_sem, device):
    return pltpu.make_async_remote_copy(
        src_ref=src,
        dst_ref=dst,
        send_sem=send_sem,
        recv_sem=recv_sem,
        device_id=device,
        device_id_type=MESH,
    )


def dot_nt(left, right):
    return lax.dot_general(
        left, right, (((1,), (1,)), ((), ())), preferred_element_type=jnp.float32
    )


def dot(left, right):
    return jnp.dot(left, right, preferred_element_type=jnp.float32)


def deltas(scaled, gate_pre, up_pre):
    sigmoid_gate = jax.nn.sigmoid(gate_pre)
    silu_gate = gate_pre * sigmoid_gate
    gate_delta = scaled * up_pre * sigmoid_gate * (1.0 + gate_pre * (1.0 - sigmoid_gate))
    return gate_delta, scaled * silu_gate, silu_gate * up_pre


def layer_kernel(
    count,
    group,
    cap,
    tok,
    cot,
    ids,
    chosen_w,
    gate_w,
    up_w,
    down_w,
    shared_gate,
    shared_up,
    shared_down,
    token_out,
    route_out,
    gate_out,
    up_out,
    down_out,
    shared_out,
    meta,
    all_meta,
    route_buf,
    route_in,
    tok_w,
    cot_w,
    col,
    cmp_send,
    cmp_in,
    pre,
    pre_other,
    turned,
    shared_turned,
    own_sum,
    other_sum,
    sum_send,
    sum_in,
    other_send,
    other_in,
    cross_send,
    cross_in,
    back_send,
    back_in,
    shared_part,
    shared_send,
    shared_in,
    pair_send,
    pair_in,
    load_sem,
    msend,
    mrecv,
    rsend,
    rrecv,
    zsend,
    zrecv,
    xsend,
    xrecv,
    dsend,
    drecv,
    osend,
    orecv,
    qsend,
    qrecv,
    bsend,
    brecv,
    ssend,
    srecv,
    own_sem,
):
    me = lax.axis_index("ep")
    mine = lax.axis_index("tp")
    level, side = lax.div(me, 2), lax.rem(me, 2)
    low = 1 - lax.div(level, LEVELS // 2)
    role = low * level + (1 - low) * (LEVELS - 1 - level)
    is_end, is_mid = role == 0, role == 1
    inner = {"ep": me + 4 * low - 2}
    outer = {"ep": me - 4 * low + 2}
    partner = {"ep": me + 1 - 2 * side}
    rows, width = tok.shape
    hid = gate_w.shape[0]
    common = shared_gate.shape[0]
    cut = width // PIECES
    every = tuple(range(PIECES))
    first, second = every[: PIECES // 2], every[PIECES // 2 :]

    def block_of(lev, column):
        return 2 * (low * lev + (1 - low) * (LEVELS - 1 - lev)) + column

    def piece(h):
        return pl.ds(h * cut, cut)

    peers = [{"ep": lax.rem(me + step, count)} for step in range(1, count)]
    near = [lax.rem(mine + step, group) for step in range(1, group)]
    greeted = greet(peers + [{"tp": to_group} for to_group in near])

    loads = [
        pltpu.make_async_copy(src, dst, load_sem.at[i])
        for i, (src, dst) in enumerate(
            (
                (tok, col.at[0, role]),
                (cot, col.at[1, role]),
                (gate_w, tok_w.at[pl.ds(0, hid)]),
                (up_w, tok_w.at[pl.ds(hid, hid)]),
                (shared_gate, tok_w.at[pl.ds(2 * hid, common)]),
                (shared_up, tok_w.at[pl.ds(2 * hid + common, common)]),
                (down_w, cot_w.at[pl.ds(0, hid)]),
                (shared_down, cot_w.at[pl.ds(hid, common)]),
            )
        )
    ]
    for copy in loads[:2]:
        copy.start()

    lane = lax.broadcasted_iota(jnp.int32, (rows, rows), 1)
    depth = lax.broadcasted_iota(jnp.int32, (rows, rows), 0)
    before = jnp.where(depth <= lane, 1.0, 0.0).astype(jnp.bfloat16)
    for expert in range(count):
        named = ids[...] == expert
        meta[expert, 0] = jnp.sum(jnp.where(named, chosen_w[...], 0.0), axis=0, keepdims=True)
        hit = jnp.sum(jnp.where(named, 1.0, 0.0), axis=0, keepdims=True)
        place = dot(jnp.broadcast_to(hit, (8, rows)).astype(jnp.bfloat16), before)[:1]
        meta[expert, 1] = jnp.where(hit > 0.0, place - 1.0, -1.0)

    greeted()

    def passed(array, lev, h, inward):
        if inward:
            lands = is_end * lev + is_mid * (LEVELS - 1 - lev)
        else:
            lands = lev
        return remote(
            col.at[array, lev, :, piece(h)],
            col.at[array, lands, :, piece(h)],
            zsend.at[1 - inward, array, lev, h],
            zrecv.at[array, lands, h],
            inner if inward else outer,
        )

    def arrival(array, lev, h):
        here = col.at[array, lev, :, piece(h)]
        return remote(here, here, zsend.at[0, array, lev, h], zrecv.at[array, lev, h], inner)

    def crossed(array, lev, h):
        return remote(
            cmp_send.at[array, lev, :, piece(h)],
            cmp_in.at[array, lev, pl.ds(0, cap), piece(h)],
            xsend.at[array, lev, h],
            xrecv.at[array, lev, h],
            partner,
        )

    def summed(lev, h):
        inward = lev > 0
        lands = is_end * lev + is_mid * (LEVELS - 1 - lev) if inward else lev
        return remote(
            sum_send.at[lev, :, piece(h)],
            sum_in.at[role, lands, :, piece(h)],
            dsend.at[lev, h],
            drecv.at[role, lands, h],
            inner if inward else outer,
        )

    def sum_wait(source, lev, h):
        remote(
            sum_send.at[lev, :, piece(h)],
            sum_in.at[source, lev, :, piece(h)],
            dsend.at[lev, h],
            drecv.at[source, lev, h],
            inner,
        ).wait_recv()

    def othered(lev, h):
        inward = lev > 0
        lands = is_end * lev + is_mid * (LEVELS - 1 - lev) if inward else lev
        return remote(
            other_send.at[lev, :, piece(h)],
            other_in.at[lands, :, piece(h)],
            osend.at[lev, h],
            orecv.at[lands, h],
            inner if inward else outer,
        )

    def other_wait(lev, h):
        remote(
            other_send.at[lev, :, piece(h)],
            other_in.at[lev, :, piece(h)],
            osend.at[lev, h],
            orecv.at[lev, h],
            inner,
        ).wait_recv()

    def over(h):
        return remote(
            cross_send.at[:, piece(h)],
            cross_in.at[:, piece(h)],
            qsend.at[h],
            qrecv.at[h],
            partner,
        )

    def returned(h):
        return remote(
            back_send.at[:, piece(h)],
            back_in.at[pl.ds(0, cap), piece(h)],
            bsend.at[h],
            brecv.at[h],
            partner,
        )

    def column_of(row):
        return jnp.sum(jnp.where(depth == lane, row, 0.0), axis=1, keepdims=True)

    def picks(row):
        return depth.astype(jnp.float32) == row

    def send_compact(array, lev, pieces):
        row = all_meta[block_of(lev, side), 1 - side, 1]
        chosen = jnp.where(picks(row), 1.0, 0.0).astype(jnp.bfloat16)[:cap]
        for h in pieces:
            cmp_send[array, lev, :, piece(h)] = dot(chosen, col[array, lev, :, piece(h)]).astype(
                jnp.bfloat16
            )
            crossed(array, lev, h).start()

    def arrive(array, lev, pieces):
        for h in pieces:
            arrival(array, lev, h).wait_recv()
            if isinstance(lev, int):
                if lev == 0:
                    passed(array, lev, h, 1).start()
                else:

                    @pl.when(is_mid)
                    def _():
                        passed(array, lev, h, 0).start()

            else:

                @pl.when(is_mid)
                def _():
                    passed(array, 0, h, 1).start()

            send_compact(array, lev, (h,))

    def send_sum(lev, pieces, source):
        for h in pieces:
            total = own_sum[lev, :, piece(h)]
            if lev == 2:
                row = all_meta[block_of(lev, side), 1 - side, 1]
                spread = jnp.where(
                    lane.astype(jnp.float32) == column_of(row), 1.0, 0.0
                ).astype(jnp.bfloat16)
                returned(h).wait_recv()
                total = total + dot(spread, back_in[:, piece(h)])
            if source is not None:
                sum_wait(source, lev, h)
                total = total + sum_in[source, lev, :, piece(h)].astype(jnp.float32)
            sum_send[lev, :, piece(h)] = total.astype(jnp.bfloat16)
            summed(lev, h).start()

    def send_other(lev, pieces, add):
        for h in pieces:
            total = other_sum[lev, :, piece(h)]
            if add:
                other_wait(lev, h)
                total = total + other_in[lev, :, piece(h)].astype(jnp.float32)
            other_send[lev, :, piece(h)] = total.astype(jnp.bfloat16)
            othered(lev, h).start()

    def send_over(pieces):
        for h in pieces:
            other_wait(role, h)
            total = other_sum[role, :, piece(h)] + other_in[role, :, piece(h)].astype(jnp.float32)
            cross_send[:, piece(h)] = total.astype(jnp.bfloat16)
            over(h).start()

    loads[0].wait()
    for h in every:
        passed(0, role, h, 1).start()

    @pl.when(is_mid)
    def _():
        for h in every:
            passed(0, 1, h, 0).start()

    loads[1].wait()

    @pl.when(is_end)
    def _():
        for h in every:
            passed(1, 0, h, 1).start()

    @pl.when(is_mid)
    def _():
        for h in every:
            passed(1, 1, h, 0).start()

    for copy in loads[2:]:
        copy.start()
    metas = []
    for step in range(1, count):
        peer = lax.rem(me + step, count)
        metas.append(
            remote(
                meta.at[pl.ds(2 * lax.div(peer, 2), 2)],
                all_meta.at[me],
                msend.at[step - 1],
                mrecv.at[step - 1],
                {"ep": peer},
            )
        )
    for copy in metas:
        copy.start()
    all_meta[me] = meta[pl.ds(2 * level, 2)]
    for array in (0, 1):
        send_compact(array, role, every)
    cmp_in[:, :, cap:] = jnp.zeros((2, LEVELS, rows - cap, width), jnp.bfloat16)
    back_in[cap:] = jnp.zeros((rows - cap, width), jnp.bfloat16)
    for copy in metas:
        copy.wait()

    def full_start(lev):
        pre[...] = dot_nt(col[0, lev], tok_w[...])

    def full(lev, head):
        block = block_of(lev, side)
        same = depth == lane
        scale = column_of(all_meta[block, side, 0])
        back_hidden = dot_nt(col[1, lev], cot_w[pl.ds(0, hid)])
        gate_pre, up_pre = pre[:, pl.ds(0, hid)], pre[:, pl.ds(hid, hid)]
        gate_delta, up_delta, hidden = deltas(scale * back_hidden, gate_pre, up_pre)
        both = jnp.concatenate([gate_delta, up_delta], axis=1).astype(jnp.bfloat16)
        own_sum[lev] = dot(both, tok_w[pl.ds(0, 2 * hid)])
        rounded = hidden.astype(jnp.bfloat16).astype(jnp.float32)
        route = jnp.sum(back_hidden * rounded, axis=1, keepdims=True)
        route_buf[block] = jnp.sum(jnp.where(same, route, 0.0), axis=0, keepdims=True)
        columns = pl.ds(pl.multiple_of(lev * rows, rows), rows)
        turned[0, :, columns] = gate_delta.T.astype(jnp.bfloat16)
        turned[1, :, columns] = up_delta.T.astype(jnp.bfloat16)
        turned[2, :, columns] = (scale * hidden).T.astype(jnp.bfloat16)
        common_back = dot_nt(col[1, lev], cot_w[pl.ds(hid, common)])
        common_gate = pre[:, pl.ds(2 * hid, common)]
        common_up = pre[:, pl.ds(2 * hid + common, common)]
        common_deltas = deltas(common_back, common_gate, common_up)
        for i in range(3):
            shared_turned[i, :, columns] = common_deltas[i].T.astype(jnp.bfloat16)

        @pl.when(head)
        def _():
            pair = jnp.concatenate(common_deltas[:2], axis=1).astype(jnp.bfloat16)
            own_sum[lev] = own_sum[lev] + dot(pair, tok_w[pl.ds(2 * hid, 2 * common)])

    def compact_start(lev):
        for h in every:
            crossed(0, lev, h).wait_recv()
        pre_other[...] = dot_nt(cmp_in[0, lev], tok_w[pl.ds(0, 2 * hid)])

    def compact(lev, last):
        for h in every:
            crossed(1, lev, h).wait_recv()
        block = block_of(lev, 1 - side)
        weight_row, row = all_meta[block, side, 0], all_meta[block, side, 1]
        chosen = picks(row)
        scale = jnp.sum(jnp.where(chosen, weight_row, 0.0), axis=1, keepdims=True)
        back_hidden = dot_nt(cmp_in[1, lev], cot_w[pl.ds(0, hid)])
        gate_pre, up_pre = pre_other[:, pl.ds(0, hid)], pre_other[:, pl.ds(hid, hid)]
        gate_delta, up_delta, hidden = deltas(scale * back_hidden, gate_pre, up_pre)
        both = jnp.concatenate([gate_delta, up_delta], axis=1).astype(jnp.bfloat16)
        target = jnp.where(last, depth.astype(jnp.float32)[:, :1], column_of(row))
        spread = jnp.where(lane.astype(jnp.float32) == target, 1.0, 0.0).astype(jnp.bfloat16)
        both = dot(spread, both).astype(jnp.bfloat16)
        for h in every:
            other_sum[lev, :, piece(h)] = dot(both, tok_w[pl.ds(0, 2 * hid), piece(h)])

            @pl.when(last)
            def _():
                back_send[:, piece(h)] = other_sum[lev, pl.ds(0, cap), piece(h)].astype(
                    jnp.bfloat16
                )
                returned(h).start()

        rounded = hidden.astype(jnp.bfloat16).astype(jnp.float32)
        route = jnp.sum(back_hidden * rounded, axis=1, keepdims=True)
        route_buf[block] = jnp.sum(jnp.where(chosen, route, 0.0), axis=0, keepdims=True)
        columns = pl.ds(pl.multiple_of((LEVELS + lev) * rows, rows), rows)
        turned[0, :, columns] = gate_delta.T.astype(jnp.bfloat16)
        turned[1, :, columns] = up_delta.T.astype(jnp.bfloat16)
        turned[2, :, columns] = (scale * hidden).T.astype(jnp.bfloat16)

    def body(i, carry):
        late = lax.div(i, 2)
        lev = (1 - late) * (i + role - 2 * i * role) + late * (5 - i)
        other_near = 1 - role

        @pl.when((i == 2) & is_end)
        def _():
            send_other(1, every, False)

        @pl.when((i == 3) & is_end)
        def _():
            send_other(3, every, False)
            arrive(0, 2, second)

        @pl.when((i == 3) & is_mid)
        def _():
            send_over(second)

        @pl.when(i == 0)
        def _():
            arrive(0, other_near, first)
            for copy in loads[2:]:
                copy.wait()

        @pl.when(i == 1)
        def _():
            arrive(1, other_near, second[:1])

        full_start(lev)

        @pl.when(i == 0)
        def _():
            arrive(0, other_near, second)

        @pl.when(i == 1)
        def _():
            arrive(1, other_near, second[1:])

            @pl.when(is_mid)
            def _():
                for h in every:
                    passed(1, 1, h, 1).start()
                arrive(0, 3, second)

        @pl.when((i == 2) & is_end)
        def _():
            arrive(1, 3, every)

        @pl.when((i == 2) & is_mid)
        def _():
            arrive(1, 2, first)

        @pl.when((i == 3) & is_end)
        def _():
            arrive(1, 2, every)

        full(lev, i == 0)

        @pl.when(i == 0)
        def _():
            arrive(1, other_near, first[:1])

        @pl.when((i == 1) & is_end)
        def _():
            send_sum(1, every, None)

        @pl.when((i == 2) & is_end)
        def _():
            send_sum(3, every, None)

        @pl.when((i == 2) & is_mid)
        def _():
            arrive(1, 2, second)

        @pl.when((i == 3) & is_mid)
        def _():
            send_sum(3, every, 0)
            send_sum(0, first, 1)
            send_other(3, first, True)

        compact_start(lev)

        @pl.when(i == 0)
        def _():
            arrive(1, other_near, first[1:])

            @pl.when(is_mid)
            def _():
                arrive(0, 3, first)

        @pl.when((i == 1) & is_end)
        def _():
            arrive(0, 3, every)

        @pl.when((i == 1) & is_mid)
        def _():
            arrive(1, 3, every)
            arrive(0, 2, every)

        @pl.when((i == 2) & is_end)
        def _():
            arrive(0, 2, first)

        @pl.when((i == 2) & is_mid)
        def _():
            send_over(first)

        compact(lev, i == LEVELS - 1)
        return carry

    lax.fori_loop(0, LEVELS, body, 0)

    @pl.when(is_mid)
    def _():
        send_sum(0, second, 1)
        send_other(3, second, True)

    routes = []
    for step in range(1, count):
        peer = lax.rem(me + step, count)
        routes.append(
            remote(
                route_buf.at[peer],
                route_in.at[me],
                rsend.at[step - 1],
                rrecv.at[step - 1],
                {"ep": peer},
            )
        )
    for copy in routes:
        copy.start()
    route_in[me] = route_buf[me]

    tile = 2 * common
    outs = (gate_out, up_out, down_out)

    def weight_grad(i):
        array = i // 2

        def tile_body(j, carry):
            cols = pl.ds(pl.multiple_of(j * tile, tile), tile)
            reach = LEVELS * rows
            grad = dot(turned[i, :, pl.ds(0, reach)], col[array, :, :, cols].reshape(reach, tile))
            grad = grad + dot(
                turned[i, :, pl.ds(reach, reach)], cmp_in[array, :, :, cols].reshape(reach, tile)
            )
            outs[i][:, cols] = grad.astype(jnp.bfloat16)
            return carry

        lax.fori_loop(0, width // tile, tile_body, 0)

    span = width // LEVELS
    size = span // (2 * group)
    mine_cols = pl.ds(pl.multiple_of(level * span, span), span)
    for i in range(3):
        block = col[i // 2, :, :, mine_cols].reshape(LEVELS * rows, span)
        grad = dot(shared_turned[i], block).T
        for to_side in range(2):
            for to_group in range(group):
                at = (to_side * group + to_group) * size
                shared_part[to_group, to_side, i] = grad[at : at + size]
                shared_send[to_group, to_side, i] = grad[at : at + size].astype(jnp.bfloat16)
    shares = [
        remote(
            shared_send.at[to_group],
            shared_in.at[mine],
            ssend.at[step],
            srecv.at[step],
            {"tp": to_group},
        )
        for step, to_group in enumerate(near)
    ]
    for copy in shares:
        copy.start()

    @pl.when(is_end)
    def _():
        send_sum(2, every, None)
        send_over(first)

    @pl.when(is_mid)
    def _():
        send_other(0, every, True)

    weight_grad(0)

    @pl.when(is_end)
    def _():
        send_over(second)

    @pl.when(is_mid)
    def _():
        send_sum(2, every, 0)

    weight_grad(1)

    for copy in shares:
        copy.wait()
    for to_side in range(2):
        total = shared_part[mine, to_side]
        for to_group in near:
            total = total + shared_in[to_group, to_side].astype(jnp.float32)
        shared_part[mine, to_side] = total
    pair_send[...] = shared_part[mine, 1 - side].astype(jnp.bfloat16)
    pair = remote(pair_send, pair_in, ssend.at[group - 1], srecv.at[group - 1], partner)
    pair.start()

    weight_grad(2)

    for copy in routes:
        copy.wait()
    found = jnp.zeros(ids.shape, jnp.float32)
    for expert in range(count):
        found = jnp.where(ids[...] == expert, route_in[expert], found)
    route_out[...] = found
    pair.wait()
    shared_out[...] = shared_part[mine, side] + pair_in[...].astype(jnp.float32)

    @pl.when(is_mid)
    def _():
        for h in every:
            sum_wait(0, 1, h)
            own_sum[1, :, piece(h)] = own_sum[1, :, piece(h)] + sum_in[0, 1, :, piece(h)].astype(
                jnp.float32
            )

    for h in every:
        sum_wait(1, role, h)
        total = own_sum[role, :, piece(h)] + sum_in[1, role, :, piece(h)].astype(jnp.float32)
        over(h).wait_recv()
        total = total + cross_in[:, piece(h)].astype(jnp.float32)
        token_out[:, piece(h)] = total.astype(jnp.bfloat16)

    def sent(*copies):
        for copy in copies:
            copy.wait_send()

    for h in every:
        sent(over(h), returned(h))
        for array in (0, 1):
            sent(passed(array, role, h, 1))
            for lev in range(LEVELS):
                sent(crossed(array, lev, h))

        @pl.when(is_end)
        def _():
            sent(summed(1, h), summed(2, h), summed(3, h), othered(1, h), othered(3, h))

        @pl.when(is_mid)
        def _():
            sent(summed(0, h), summed(2, h), summed(3, h), othered(0, h), othered(3, h))
            for array in (0, 1):
                sent(passed(array, 0, h, 1))
                for lev in (1, 2, 3):
                    sent(passed(array, lev, h, 0))


def layer(tokens, cotangent, ids, weights, experts, commons, count, group, cap):
    rows, width = tokens.shape
    hid, common = experts[0].shape[0], commons[0].shape[0]
    piece = width // count // group
    vmem = pl.BlockSpec(memory_space=pltpu.VMEM)
    anywhere = pl.BlockSpec(memory_space=pl.ANY)
    grad = pltpu.VMEM((hid, width), jnp.bfloat16)
    shared = (3, piece, common)
    bf16, f32, dma = jnp.bfloat16, jnp.float32, pltpu.SemaphoreType.DMA
    return pl.pallas_call(
        functools.partial(layer_kernel, count, group, cap),
        out_shape=(
            pltpu.VMEM((rows, width), bf16),
            pltpu.VMEM(ids.shape, f32),
            grad,
            grad,
            grad,
            pltpu.VMEM(shared, f32),
        ),
        in_specs=[anywhere, anywhere, vmem, vmem] + [anywhere] * 6,
        out_specs=(vmem,) * 6,
        scratch_shapes=[
            pltpu.VMEM((count, 2, 1, rows), f32),
            pltpu.VMEM((count, 2, 2, 1, rows), f32),
            pltpu.VMEM((count, 1, rows), f32),
            pltpu.VMEM((count, 1, rows), f32),
            pltpu.VMEM((2 * hid + 2 * common, width), bf16),
            pltpu.VMEM((hid + common, width), bf16),
            pltpu.VMEM((2, LEVELS, rows, width), bf16),
            pltpu.VMEM((2, LEVELS, cap, width), bf16),
            pltpu.VMEM((2, LEVELS, rows, width), bf16),
            pltpu.VMEM((rows, 2 * hid + 2 * common), f32),
            pltpu.VMEM((rows, 2 * hid), f32),
            pltpu.VMEM((3, hid, 2 * LEVELS * rows), bf16),
            pltpu.VMEM((3, common, LEVELS * rows), bf16),
            pltpu.VMEM((LEVELS, rows, width), f32),
            pltpu.VMEM((LEVELS, rows, width), f32),
            pltpu.VMEM((LEVELS, rows, width), bf16),
            pltpu.VMEM((2, LEVELS, rows, width), bf16),
            pltpu.VMEM((LEVELS, rows, width), bf16),
            pltpu.VMEM((LEVELS, rows, width), bf16),
            pltpu.VMEM((rows, width), bf16),
            pltpu.VMEM((rows, width), bf16),
            pltpu.VMEM((cap, width), bf16),
            pltpu.VMEM((rows, width), bf16),
            pltpu.VMEM((group, 2) + shared, f32),
            pltpu.VMEM((group, 2) + shared, bf16),
            pltpu.VMEM((group, 2) + shared, bf16),
            pltpu.VMEM(shared, bf16),
            pltpu.VMEM(shared, bf16),
            dma((8,)),
            dma((count - 1,)),
            dma((count - 1,)),
            dma((count - 1,)),
            dma((count - 1,)),
            dma((2, 2, LEVELS, PIECES)),
            dma((2, LEVELS, PIECES)),
            dma((2, LEVELS, PIECES)),
            dma((2, LEVELS, PIECES)),
            dma((LEVELS, PIECES)),
            dma((2, LEVELS, PIECES)),
            dma((LEVELS, PIECES)),
            dma((LEVELS, PIECES)),
            dma((PIECES,)),
            dma((PIECES,)),
            dma((PIECES,)),
            dma((PIECES,)),
            dma((group,)),
            dma((group,)),
            dma((2,)),
        ],
        compiler_params=pltpu.CompilerParams(
            collective_id=0, has_side_effects=True, vmem_limit_bytes=55 * 2**20
        ),
    )(tokens, cotangent, ids, weights, *experts, *commons)


def flush_kernel(count, *refs):
    copies = [
        pltpu.make_async_copy(refs[i], refs[count + i], refs[2 * count].at[i]) for i in range(count)
    ]
    for copy in copies:
        copy.start()
    for copy in copies:
        copy.wait()


def flush(*held):
    count = len(held)
    return pl.pallas_call(
        functools.partial(flush_kernel, count),
        out_shape=tuple(jax.ShapeDtypeStruct(x.shape, x.dtype) for x in held),
        in_specs=[pl.BlockSpec(memory_space=pltpu.VMEM)] * count,
        out_specs=(pl.BlockSpec(memory_space=pl.ANY),) * count,
        scratch_shapes=[pltpu.SemaphoreType.DMA((count,))],
        compiler_params=pltpu.CompilerParams(vmem_limit_bytes=2**20),
    )(*held)


def gathered_shards(
    tokens,
    expert_ids,
    route_weights,
    cotangent,
    gate_weight,
    up_weight,
    down_weight,
    shared_gate,
    shared_up,
    shared_down,
):
    count, group = lax.axis_size("ep"), lax.axis_size("tp")
    held = layer(
        tokens,
        cotangent,
        expert_ids.T,
        route_weights.T,
        (gate_weight[0], up_weight[0], down_weight[0]),
        (shared_gate, shared_up, shared_down),
        count,
        group,
        3 * tokens.shape[0] * expert_ids.shape[1] // (2 * count),
    )
    token_grad, route_grad, gate_grad, up_grad, down_grad, shared_sum = flush(*held)
    return (
        token_grad,
        route_grad.T,
        gate_grad[None],
        up_grad[None],
        down_grad[None],
        jnp.transpose(shared_sum, (1, 0, 2)),
    )


def shards(tokens, expert_ids, *rest):
    dense = 2 * LEVELS == lax.axis_size("ep") <= 2 * expert_ids.shape[1]
    return (gathered_shards if dense else exchanged_shards)(tokens, expert_ids, *rest)


def solution(mesh):
    in_specs = (
        P(("ep", "tp"), None),
        P(("ep", "tp"), None),
        P(("ep", "tp"), None),
        P(("ep", "tp"), None),
        P(("ep", "tp"), None, None),
        P(("ep", "tp"), None, None),
        P(("ep", "tp"), None, None),
        P(),
        P(),
        P(),
    )
    out_specs = (
        P(("ep", "tp"), None),
        P(("ep", "tp"), None),
        P(("ep", "tp"), None, None),
        P(("ep", "tp"), None, None),
        P(("ep", "tp"), None, None),
        P(("ep", "tp"), None, None),
    )
    return jax.shard_map(shards, mesh=mesh, in_specs=in_specs, out_specs=out_specs, check_vma=False)
```

```python
import functools

import jax
import jax.numpy as jnp
from jax import lax
from jax.experimental import pallas as pl
from jax.experimental.pallas import tpu as pltpu
from jax.sharding import PartitionSpec as P


def gated_backward(scaled, gate_pre, up_pre):
    sigmoid_gate = jax.nn.sigmoid(gate_pre)
    gate_delta = (scaled * up_pre * sigmoid_gate * (1.0 + gate_pre * (1.0 - sigmoid_gate))).astype(
        jnp.bfloat16
    )
    up_delta = (scaled * jax.nn.silu(gate_pre)).astype(jnp.bfloat16)
    return (gate_delta, up_delta)


def forward_products(token_rows, gate_local, up_local):
    gate_pre = jnp.einsum("rd,fd->rf", token_rows, gate_local, preferred_element_type=jnp.float32)
    up_pre = jnp.einsum("rd,fd->rf", token_rows, up_local, preferred_element_type=jnp.float32)
    return (gate_pre, up_pre)


def exchanged_shards(
    tokens,
    expert_ids,
    route_weights,
    cotangent,
    gate_weight,
    up_weight,
    down_weight,
    shared_gate,
    shared_up,
    shared_down,
):
    ep_size = lax.axis_size("ep")
    tok_rows = tokens.shape[0]
    model_width = tokens.shape[1]
    top_count = expert_ids.shape[1]
    capacity = 3 * tok_rows * top_count // (2 * ep_size)
    slots_all = ep_size * capacity
    assign_count = tok_rows * top_count
    flat_ids = expert_ids.reshape(-1)
    one_hot = (flat_ids[:, None] == jnp.arange(ep_size, dtype=jnp.int32)[None, :]).astype(jnp.int32)
    slot_index = jnp.sum(jnp.cumsum(one_hot, axis=0) * one_hot, axis=1) - 1
    position = flat_ids * capacity + slot_index
    row_assign = (
        jnp.full((slots_all,), assign_count, jnp.int32)
        .at[position]
        .set(jnp.arange(assign_count, dtype=jnp.int32))
    )
    row_token = row_assign // top_count
    row_weight = jnp.take(
        jnp.concatenate([route_weights.reshape(-1), jnp.zeros((1,), jnp.float32)], axis=0),
        row_assign,
        axis=0,
    )
    empty_row = jnp.zeros((1, model_width), jnp.bfloat16)
    send_tokens = jnp.take(jnp.concatenate([tokens, empty_row], axis=0), row_token, axis=0).reshape(
        ep_size, capacity, model_width
    )
    send_cot = jnp.take(jnp.concatenate([cotangent, empty_row], axis=0), row_token, axis=0).reshape(
        ep_size, capacity, model_width
    )
    gate_local = gate_weight[0]
    up_local = up_weight[0]
    down_local = down_weight[0]
    scales = lax.all_to_all(
        row_weight.reshape(ep_size, capacity), "ep", split_axis=0, concat_axis=0, tiled=True
    ).reshape(slots_all)
    token_rows, cot_rows = (
        lax.all_to_all(send_tokens, "ep", split_axis=0, concat_axis=0, tiled=True),
        lax.all_to_all(send_cot, "ep", split_axis=0, concat_axis=0, tiled=True),
    )
    token_rows = token_rows.reshape(slots_all, model_width)
    cot_rows = cot_rows.reshape(slots_all, model_width)
    gate_pre, up_pre = forward_products(token_rows, gate_local, up_local)
    hidden = (jax.nn.silu(gate_pre) * up_pre).astype(jnp.bfloat16)
    back_hidden = jnp.einsum("rd,fd->rf", cot_rows, down_local, preferred_element_type=jnp.float32)
    route_part = jnp.sum(back_hidden * hidden.astype(jnp.float32), axis=1)
    gate_delta, up_delta = gated_backward(scales[:, None] * back_hidden, gate_pre, up_pre)
    weighted_cot = (scales[:, None] * cot_rows.astype(jnp.float32)).astype(jnp.bfloat16)
    token_part = jnp.einsum(
        "rf,fd->rd", gate_delta, gate_local, preferred_element_type=jnp.float32
    ) + jnp.einsum("rf,fd->rd", up_delta, up_local, preferred_element_type=jnp.float32)
    gate_grad = jnp.einsum(
        "rf,rd->fd", gate_delta, token_rows, preferred_element_type=jnp.float32
    ).astype(jnp.bfloat16)[None]
    up_grad = jnp.einsum(
        "rf,rd->fd", up_delta, token_rows, preferred_element_type=jnp.float32
    ).astype(jnp.bfloat16)[None]
    down_grad = jnp.einsum(
        "rf,rd->fd", hidden, weighted_cot, preferred_element_type=jnp.float32
    ).astype(jnp.bfloat16)[None]
    back_rows, back_route = (
        lax.all_to_all(
            token_part.reshape(ep_size, capacity, model_width),
            "ep",
            split_axis=0,
            concat_axis=0,
            tiled=True,
        ),
        lax.all_to_all(
            route_part.reshape(ep_size, capacity), "ep", split_axis=0, concat_axis=0, tiled=True
        ),
    )
    routed = jnp.sum(
        jnp.take(back_rows.reshape(slots_all, model_width), position, axis=0).reshape(
            tok_rows, top_count, model_width
        ),
        axis=1,
    )
    route_grad = jnp.take(back_route.reshape(slots_all), position, axis=0).reshape(
        tok_rows, top_count
    )
    common_gate = jnp.einsum("td,fd->tf", tokens, shared_gate, preferred_element_type=jnp.float32)
    common_up = jnp.einsum("td,fd->tf", tokens, shared_up, preferred_element_type=jnp.float32)
    common_hidden = (jax.nn.silu(common_gate) * common_up).astype(jnp.bfloat16)
    common_back = jnp.einsum(
        "td,fd->tf", cotangent, shared_down, preferred_element_type=jnp.float32
    )
    common_gate_delta, common_up_delta = gated_backward(common_back, common_gate, common_up)
    common_part = jnp.einsum(
        "tf,fd->td", common_gate_delta, shared_gate, preferred_element_type=jnp.float32
    ) + jnp.einsum("tf,fd->td", common_up_delta, shared_up, preferred_element_type=jnp.float32)
    shared_grads = lax.psum_scatter(
        jnp.stack(
            [
                jnp.einsum(
                    "tc,tf->cf", tokens, common_gate_delta, preferred_element_type=jnp.float32
                ),
                jnp.einsum(
                    "tc,tf->cf", tokens, common_up_delta, preferred_element_type=jnp.float32
                ),
                jnp.einsum(
                    "tc,tf->cf", cotangent, common_hidden, preferred_element_type=jnp.float32
                ),
            ],
            axis=1,
        ),
        ("ep", "tp"),
        scatter_dimension=0,
        tiled=True,
    )
    token_grad = (routed + common_part).astype(jnp.bfloat16)
    return (token_grad, route_grad, gate_grad, up_grad, down_grad, shared_grads)


MESH = pl.DeviceIdType.MESH
LEVELS = 4
PIECES = 4


def greet(peers):
    barrier = pltpu.get_barrier_semaphore()
    for peer in peers:
        pl.semaphore_signal(barrier, inc=1, device_id=peer, device_id_type=MESH)
    return lambda: pl.semaphore_wait(barrier, len(peers))


def remote(src, dst, send_sem, recv_sem, device):
    return pltpu.make_async_remote_copy(
        src_ref=src,
        dst_ref=dst,
        send_sem=send_sem,
        recv_sem=recv_sem,
        device_id=device,
        device_id_type=MESH,
    )


def dot_nt(left, right):
    return lax.dot_general(
        left, right, (((1,), (1,)), ((), ())), preferred_element_type=jnp.float32
    )


def dot(left, right):
    return jnp.dot(left, right, preferred_element_type=jnp.float32)


def deltas(scaled, gate_pre, up_pre):
    sigmoid_gate = jax.nn.sigmoid(gate_pre)
    silu_gate = gate_pre * sigmoid_gate
    gate_delta = scaled * up_pre * sigmoid_gate * (1.0 + gate_pre * (1.0 - sigmoid_gate))
    return gate_delta, scaled * silu_gate, silu_gate * up_pre


def layer_kernel(
    count,
    group,
    cap,
    tok,
    cot,
    ids_from,
    chosen_from,
    gate_w,
    up_w,
    down_w,
    shared_gate,
    shared_up,
    shared_down,
    token_out,
    route_out,
    gate_out,
    up_out,
    down_out,
    shared_out,
    ids,
    chosen_w,
    meta,
    all_meta,
    route_buf,
    route_in,
    tok_w,
    cot_w,
    col,
    cmp_send,
    cmp_in,
    pre,
    pre_other,
    turned,
    shared_turned,
    own_sum,
    other_sum,
    sum_send,
    sum_in,
    other_send,
    other_in,
    cross_send,
    cross_in,
    back_send,
    back_in,
    shared_part,
    shared_send,
    shared_in,
    pair_send,
    pair_in,
    load_sem,
    msend,
    mrecv,
    rsend,
    rrecv,
    zsend,
    zrecv,
    xsend,
    xrecv,
    dsend,
    drecv,
    osend,
    orecv,
    qsend,
    qrecv,
    bsend,
    brecv,
    ssend,
    srecv,
    own_sem,
):
    me = lax.axis_index("ep")
    mine = lax.axis_index("tp")
    level, side = lax.div(me, 2), lax.rem(me, 2)
    low = 1 - lax.div(level, LEVELS // 2)
    role = low * level + (1 - low) * (LEVELS - 1 - level)
    is_end, is_mid = role == 0, role == 1
    inner = {"ep": me + 4 * low - 2}
    outer = {"ep": me - 4 * low + 2}
    partner = {"ep": me + 1 - 2 * side}
    rows, width = tok.shape
    hid = gate_w.shape[0]
    common = shared_gate.shape[0]
    cut = width // PIECES
    every = tuple(range(PIECES))
    first, second = every[: PIECES // 2], every[PIECES // 2 :]

    def block_of(lev, column):
        return 2 * (low * lev + (1 - low) * (LEVELS - 1 - lev)) + column

    def piece(h):
        return pl.ds(h * cut, cut)

    peers = [{"ep": lax.rem(me + step, count)} for step in range(1, count)]
    near = [lax.rem(mine + step, group) for step in range(1, group)]
    greeted = greet(peers + [{"tp": to_group} for to_group in near])

    loads = [
        pltpu.make_async_copy(src, dst, load_sem.at[i])
        for i, (src, dst) in enumerate(
            (
                (tok, col.at[0, role]),
                (cot, col.at[1, role]),
                (ids_from, ids),
                (chosen_from, chosen_w),
                (gate_w, tok_w.at[pl.ds(0, hid)]),
                (up_w, tok_w.at[pl.ds(hid, hid)]),
                (shared_gate, tok_w.at[pl.ds(2 * hid, common)]),
                (shared_up, tok_w.at[pl.ds(2 * hid + common, common)]),
                (down_w, cot_w.at[pl.ds(0, hid)]),
                (shared_down, cot_w.at[pl.ds(hid, common)]),
            )
        )
    ]
    for copy in loads[2:4] + loads[:2]:
        copy.start()
    for copy in loads[2:4]:
        copy.wait()

    lane = lax.broadcasted_iota(jnp.int32, (rows, rows), 1)
    depth = lax.broadcasted_iota(jnp.int32, (rows, rows), 0)
    before = jnp.where(depth <= lane, 1.0, 0.0).astype(jnp.bfloat16)
    for expert in range(count):
        named = ids[...] == expert
        meta[expert, 0] = jnp.sum(jnp.where(named, chosen_w[...], 0.0), axis=0, keepdims=True)
        hit = jnp.sum(jnp.where(named, 1.0, 0.0), axis=0, keepdims=True)
        place = dot(jnp.broadcast_to(hit, (8, rows)).astype(jnp.bfloat16), before)[:1]
        meta[expert, 1] = jnp.where(hit > 0.0, place - 1.0, -1.0)

    greeted()

    def passed(array, lev, h, inward):
        if inward:
            lands = is_end * lev + is_mid * (LEVELS - 1 - lev)
        else:
            lands = lev
        return remote(
            col.at[array, lev, :, piece(h)],
            col.at[array, lands, :, piece(h)],
            zsend.at[1 - inward, array, lev, h],
            zrecv.at[array, lands, h],
            inner if inward else outer,
        )

    def arrival(array, lev, h):
        here = col.at[array, lev, :, piece(h)]
        return remote(here, here, zsend.at[0, array, lev, h], zrecv.at[array, lev, h], inner)

    def crossed(array, lev, h):
        return remote(
            cmp_send.at[array, lev, :, piece(h)],
            cmp_in.at[array, lev, pl.ds(0, cap), piece(h)],
            xsend.at[array, lev, h],
            xrecv.at[array, lev, h],
            partner,
        )

    def summed(lev, h):
        inward = lev > 0
        lands = is_end * lev + is_mid * (LEVELS - 1 - lev) if inward else lev
        return remote(
            sum_send.at[lev, :, piece(h)],
            sum_in.at[role, lands, :, piece(h)],
            dsend.at[lev, h],
            drecv.at[role, lands, h],
            inner if inward else outer,
        )

    def sum_wait(source, lev, h):
        remote(
            sum_send.at[lev, :, piece(h)],
            sum_in.at[source, lev, :, piece(h)],
            dsend.at[lev, h],
            drecv.at[source, lev, h],
            inner,
        ).wait_recv()

    def othered(lev, h):
        inward = lev > 0
        lands = is_end * lev + is_mid * (LEVELS - 1 - lev) if inward else lev
        return remote(
            other_send.at[lev, :, piece(h)],
            other_in.at[lands, :, piece(h)],
            osend.at[lev, h],
            orecv.at[lands, h],
            inner if inward else outer,
        )

    def other_wait(lev, h):
        remote(
            other_send.at[lev, :, piece(h)],
            other_in.at[lev, :, piece(h)],
            osend.at[lev, h],
            orecv.at[lev, h],
            inner,
        ).wait_recv()

    def over(h):
        return remote(
            cross_send.at[:, piece(h)],
            cross_in.at[:, piece(h)],
            qsend.at[h],
            qrecv.at[h],
            partner,
        )

    def returned(h):
        return remote(
            back_send.at[:, piece(h)],
            back_in.at[pl.ds(0, cap), piece(h)],
            bsend.at[h],
            brecv.at[h],
            partner,
        )

    def column_of(row):
        return jnp.sum(jnp.where(depth == lane, row, 0.0), axis=1, keepdims=True)

    def picks(row):
        return depth.astype(jnp.float32) == row

    def send_compact(array, lev, pieces):
        row = all_meta[block_of(lev, side), 1 - side, 1]
        chosen = jnp.where(picks(row), 1.0, 0.0).astype(jnp.bfloat16)[:cap]
        for h in pieces:
            cmp_send[array, lev, :, piece(h)] = dot(chosen, col[array, lev, :, piece(h)]).astype(
                jnp.bfloat16
            )
            crossed(array, lev, h).start()

    def arrive(array, lev, pieces):
        for h in pieces:
            arrival(array, lev, h).wait_recv()
            if isinstance(lev, int):
                if lev == 0:
                    passed(array, lev, h, 1).start()
                else:

                    @pl.when(is_mid)
                    def _():
                        passed(array, lev, h, 0).start()

            else:

                @pl.when(is_mid)
                def _():
                    passed(array, 0, h, 1).start()

            send_compact(array, lev, (h,))

    def send_sum(lev, pieces, source):
        if lev == 2:
            row = all_meta[block_of(lev, side), 1 - side, 1]
            spread = jnp.where(
                lane.astype(jnp.float32) == column_of(row), 1.0, 0.0
            ).astype(jnp.bfloat16)
        for h in pieces:
            total = own_sum[lev, :, piece(h)]
            if lev == 2:
                returned(h).wait_recv()
                total = total + dot(spread, back_in[:, piece(h)])
            if source is not None:
                sum_wait(source, lev, h)
                total = total + sum_in[source, lev, :, piece(h)].astype(jnp.float32)
            sum_send[lev, :, piece(h)] = total.astype(jnp.bfloat16)
            summed(lev, h).start()

    def send_other(lev, pieces, add):
        for h in pieces:
            total = other_sum[lev, :, piece(h)]
            if add:
                other_wait(lev, h)
                total = total + other_in[lev, :, piece(h)].astype(jnp.float32)
            other_send[lev, :, piece(h)] = total.astype(jnp.bfloat16)
            othered(lev, h).start()

    def send_over(pieces):
        for h in pieces:
            other_wait(role, h)
            total = other_sum[role, :, piece(h)] + other_in[role, :, piece(h)].astype(jnp.float32)
            cross_send[:, piece(h)] = total.astype(jnp.bfloat16)
            over(h).start()

    loads[0].wait()
    for h in every:
        passed(0, role, h, 1).start()

    @pl.when(is_mid)
    def _():
        for h in every:
            passed(0, 1, h, 0).start()

    loads[1].wait()

    @pl.when(is_end)
    def _():
        for h in every:
            passed(1, 0, h, 1).start()

    @pl.when(is_mid)
    def _():
        for h in every:
            passed(1, 1, h, 0).start()

    for copy in loads[4:]:
        copy.start()
    metas = []
    for step in range(1, count):
        peer = lax.rem(me + step, count)
        metas.append(
            remote(
                meta.at[pl.ds(2 * lax.div(peer, 2), 2)],
                all_meta.at[me],
                msend.at[step - 1],
                mrecv.at[step - 1],
                {"ep": peer},
            )
        )
    for copy in metas:
        copy.start()
    all_meta[me] = meta[pl.ds(2 * level, 2)]
    for array in (0, 1):
        send_compact(array, role, every)
    cmp_in[:, :, cap:] = jnp.zeros((2, LEVELS, rows - cap, width), jnp.bfloat16)
    back_in[cap:] = jnp.zeros((rows - cap, width), jnp.bfloat16)
    for copy in metas:
        copy.wait()

    def full_start(lev):
        pre[...] = dot_nt(col[0, lev], tok_w[...])

    def full(lev, head):
        block = block_of(lev, side)
        same = depth == lane
        scale = column_of(all_meta[block, side, 0])
        back_hidden = dot_nt(col[1, lev], cot_w[pl.ds(0, hid)])
        gate_pre, up_pre = pre[:, pl.ds(0, hid)], pre[:, pl.ds(hid, hid)]
        gate_delta, up_delta, hidden = deltas(scale * back_hidden, gate_pre, up_pre)
        both = jnp.concatenate([gate_delta, up_delta], axis=1).astype(jnp.bfloat16)
        own_sum[lev] = dot(both, tok_w[pl.ds(0, 2 * hid)])

        def rest():
            rounded = hidden.astype(jnp.bfloat16).astype(jnp.float32)
            route = jnp.sum(back_hidden * rounded, axis=1, keepdims=True)
            route_buf[block] = jnp.sum(jnp.where(same, route, 0.0), axis=0, keepdims=True)
            columns = pl.ds(pl.multiple_of(lev * rows, rows), rows)
            turned[0, :, columns] = gate_delta.T.astype(jnp.bfloat16)
            turned[1, :, columns] = up_delta.T.astype(jnp.bfloat16)
            turned[2, :, columns] = (scale * hidden).T.astype(jnp.bfloat16)
            common_back = dot_nt(col[1, lev], cot_w[pl.ds(hid, common)])
            common_gate = pre[:, pl.ds(2 * hid, common)]
            common_up = pre[:, pl.ds(2 * hid + common, common)]
            common_deltas = deltas(common_back, common_gate, common_up)
            for i in range(3):
                shared_turned[i, :, columns] = common_deltas[i].T.astype(jnp.bfloat16)

            @pl.when(head)
            def _():
                pair = jnp.concatenate(common_deltas[:2], axis=1).astype(jnp.bfloat16)
                own_sum[lev] = own_sum[lev] + dot(pair, tok_w[pl.ds(2 * hid, 2 * common)])

        return rest

    def compact_start(lev):
        for h in every:
            crossed(0, lev, h).wait_recv()
        pre_other[...] = dot_nt(cmp_in[0, lev], tok_w[pl.ds(0, 2 * hid)])

    def compact(lev, last):
        for h in every:
            crossed(1, lev, h).wait_recv()
        block = block_of(lev, 1 - side)
        weight_row, row = all_meta[block, side, 0], all_meta[block, side, 1]
        chosen = picks(row)
        scale = jnp.sum(jnp.where(chosen, weight_row, 0.0), axis=1, keepdims=True)
        back_hidden = dot_nt(cmp_in[1, lev], cot_w[pl.ds(0, hid)])
        gate_pre, up_pre = pre_other[:, pl.ds(0, hid)], pre_other[:, pl.ds(hid, hid)]
        gate_delta, up_delta, hidden = deltas(scale * back_hidden, gate_pre, up_pre)
        both = jnp.concatenate([gate_delta, up_delta], axis=1).astype(jnp.bfloat16)
        target = jnp.where(last, depth.astype(jnp.float32)[:, :1], column_of(row))
        spread = jnp.where(lane.astype(jnp.float32) == target, 1.0, 0.0).astype(jnp.bfloat16)
        both = dot(spread, both).astype(jnp.bfloat16)
        for h in every:
            other_sum[lev, :, piece(h)] = dot(both, tok_w[pl.ds(0, 2 * hid), piece(h)])

            @pl.when(last)
            def _():
                back_send[:, piece(h)] = other_sum[lev, pl.ds(0, cap), piece(h)].astype(
                    jnp.bfloat16
                )
                returned(h).start()

        def rest():
            rounded = hidden.astype(jnp.bfloat16).astype(jnp.float32)
            route = jnp.sum(back_hidden * rounded, axis=1, keepdims=True)
            route_buf[block] = jnp.sum(jnp.where(chosen, route, 0.0), axis=0, keepdims=True)
            columns = pl.ds(pl.multiple_of((LEVELS + lev) * rows, rows), rows)
            turned[0, :, columns] = gate_delta.T.astype(jnp.bfloat16)
            turned[1, :, columns] = up_delta.T.astype(jnp.bfloat16)
            turned[2, :, columns] = (scale * hidden).T.astype(jnp.bfloat16)

        return rest

    def body(i, carry):
        late = lax.div(i, 2)
        lev = (1 - late) * (i + role - 2 * i * role) + late * (5 - i)
        other_near = 1 - role

        @pl.when((i == 3) & is_end)
        def _():
            arrive(0, 2, second)

        @pl.when((i == 3) & is_mid)
        def _():
            send_over(second)

        @pl.when(i == 0)
        def _():
            arrive(0, other_near, first)
            for copy in loads[4:]:
                copy.wait()

        @pl.when(i == 1)
        def _():
            arrive(1, other_near, second[:1])

        full_start(lev)

        @pl.when(i == 0)
        def _():
            arrive(0, other_near, second)

        @pl.when(i == 1)
        def _():
            arrive(1, other_near, second[1:])

            @pl.when(is_mid)
            def _():
                for h in every:
                    passed(1, 1, h, 1).start()
                arrive(0, 3, second)

        @pl.when((i == 2) & is_end)
        def _():
            arrive(1, 3, every)

        @pl.when((i == 2) & is_mid)
        def _():
            arrive(1, 2, first)

        @pl.when((i == 3) & is_end)
        def _():
            arrive(1, 2, every)

        @pl.when((i == 3) & is_mid)
        def _():
            send_sum(3, first, 0)

        rest = full(lev, i == 0)

        @pl.when((i == 1) & is_end)
        def _():
            send_sum(1, every, None)

        @pl.when((i == 2) & is_end)
        def _():
            send_sum(3, every, None)

        rest()

        @pl.when(i == 0)
        def _():
            arrive(1, other_near, first[:1])

        @pl.when((i == 2) & is_mid)
        def _():
            arrive(1, 2, second)

        @pl.when((i == 3) & is_mid)
        def _():
            send_sum(3, second, 0)
            send_sum(0, first, 1)
            send_other(3, first, True)

        compact_start(lev)

        @pl.when(i == 0)
        def _():
            arrive(1, other_near, first[1:])

            @pl.when(is_mid)
            def _():
                arrive(0, 3, first)

        @pl.when((i == 1) & is_end)
        def _():
            arrive(0, 3, every)

        @pl.when((i == 1) & is_mid)
        def _():
            arrive(1, 3, every)
            arrive(0, 2, every)

        @pl.when((i == 2) & is_end)
        def _():
            arrive(0, 2, first)

        @pl.when((i == 2) & is_mid)
        def _():
            send_over(first)

        rest = compact(lev, i == LEVELS - 1)

        @pl.when((i == 1) & is_end)
        def _():
            send_other(1, every, False)

        @pl.when((i == 2) & is_end)
        def _():
            send_other(3, every, False)

        rest()
        return carry

    lax.fori_loop(0, LEVELS, body, 0)

    @pl.when(is_mid)
    def _():
        send_sum(0, second, 1)
        send_other(3, second, True)

    routes = []
    for step in range(1, count):
        peer = lax.rem(me + step, count)
        routes.append(
            remote(
                route_buf.at[peer],
                route_in.at[me],
                rsend.at[step - 1],
                rrecv.at[step - 1],
                {"ep": peer},
            )
        )
    for copy in routes:
        copy.start()
    route_in[me] = route_buf[me]

    tile = 2 * common
    outs = (gate_out, up_out, down_out)

    def weight_grad(i):
        array = i // 2

        def tile_body(j, carry):
            cols = pl.ds(pl.multiple_of(j * tile, tile), tile)
            reach = LEVELS * rows
            grad = dot(turned[i, :, pl.ds(0, reach)], col[array, :, :, cols].reshape(reach, tile))
            grad = grad + dot(
                turned[i, :, pl.ds(reach, reach)], cmp_in[array, :, :, cols].reshape(reach, tile)
            )
            outs[i][:, cols] = grad.astype(jnp.bfloat16)
            return carry

        lax.fori_loop(0, width // tile, tile_body, 0)

    span = width // LEVELS
    size = span // (2 * group)
    mine_cols = pl.ds(pl.multiple_of(level * span, span), span)
    for i in range(3):
        block = col[i // 2, :, :, mine_cols].reshape(LEVELS * rows, span)
        grad = dot(shared_turned[i], block).T
        for to_side in range(2):
            for to_group in range(group):
                at = (to_side * group + to_group) * size
                shared_part[to_group, to_side, i] = grad[at : at + size]
                shared_send[to_group, to_side, i] = grad[at : at + size].astype(jnp.bfloat16)
    shares = [
        remote(
            shared_send.at[to_group],
            shared_in.at[mine],
            ssend.at[step],
            srecv.at[step],
            {"tp": to_group},
        )
        for step, to_group in enumerate(near)
    ]
    for copy in shares:
        copy.start()

    @pl.when(is_mid)
    def _():
        send_other(0, every, True)

    weight_grad(0)

    @pl.when(is_end)
    def _():
        send_sum(2, every, None)
        send_over(first)

    @pl.when(is_mid)
    def _():
        send_sum(2, every, 0)

    @pl.when(is_mid)
    def _():
        for h in every:
            sum_wait(0, 1, h)
            own_sum[1, :, piece(h)] = own_sum[1, :, piece(h)] + sum_in[0, 1, :, piece(h)].astype(
                jnp.float32
            )

    weight_grad(1)

    @pl.when(is_end)
    def _():
        send_over(second)

    for copy in shares:
        copy.wait()
    for to_side in range(2):
        total = shared_part[mine, to_side]
        for to_group in near:
            total = total + shared_in[to_group, to_side].astype(jnp.float32)
        shared_part[mine, to_side] = total
    pair_send[...] = shared_part[mine, 1 - side].astype(jnp.bfloat16)
    pair = remote(pair_send, pair_in, ssend.at[group - 1], srecv.at[group - 1], partner)
    pair.start()

    weight_grad(2)

    for copy in routes:
        copy.wait()
    found = jnp.zeros(ids.shape, jnp.float32)
    for expert in range(count):
        found = jnp.where(ids[...] == expert, route_in[expert], found)
    route_out[...] = found
    pair.wait()
    shared_out[...] = shared_part[mine, side] + pair_in[...].astype(jnp.float32)

    for h in every:
        sum_wait(1, role, h)
        total = own_sum[role, :, piece(h)] + sum_in[1, role, :, piece(h)].astype(jnp.float32)
        over(h).wait_recv()
        total = total + cross_in[:, piece(h)].astype(jnp.float32)
        token_out[:, piece(h)] = total.astype(jnp.bfloat16)

    def sent(*copies):
        for copy in copies:
            copy.wait_send()

    for h in every:
        sent(over(h), returned(h))
        for array in (0, 1):
            sent(passed(array, role, h, 1))
            for lev in range(LEVELS):
                sent(crossed(array, lev, h))

        @pl.when(is_end)
        def _():
            sent(summed(1, h), summed(2, h), summed(3, h), othered(1, h), othered(3, h))

        @pl.when(is_mid)
        def _():
            sent(summed(0, h), summed(2, h), summed(3, h), othered(0, h), othered(3, h))
            for array in (0, 1):
                sent(passed(array, 0, h, 1))
                for lev in (1, 2, 3):
                    sent(passed(array, lev, h, 0))


def layer(tokens, cotangent, ids, weights, experts, commons, count, group, cap):
    rows, width = tokens.shape
    hid, common = experts[0].shape[0], commons[0].shape[0]
    piece = width // count // group
    vmem = pl.BlockSpec(memory_space=pltpu.VMEM)
    anywhere = pl.BlockSpec(memory_space=pl.ANY)
    grad = pltpu.VMEM((hid, width), jnp.bfloat16)
    shared = (3, piece, common)
    bf16, f32, dma = jnp.bfloat16, jnp.float32, pltpu.SemaphoreType.DMA
    return pl.pallas_call(
        functools.partial(layer_kernel, count, group, cap),
        out_shape=(
            pltpu.VMEM((rows, width), bf16),
            pltpu.VMEM(ids.shape, f32),
            grad,
            grad,
            grad,
            pltpu.VMEM(shared, f32),
        ),
        in_specs=[anywhere] * 10,
        out_specs=(vmem,) * 6,
        scratch_shapes=[
            pltpu.VMEM(ids.shape, ids.dtype),
            pltpu.VMEM(weights.shape, weights.dtype),
            pltpu.VMEM((count, 2, 1, rows), f32),
            pltpu.VMEM((count, 2, 2, 1, rows), f32),
            pltpu.VMEM((count, 1, rows), f32),
            pltpu.VMEM((count, 1, rows), f32),
            pltpu.VMEM((2 * hid + 2 * common, width), bf16),
            pltpu.VMEM((hid + common, width), bf16),
            pltpu.VMEM((2, LEVELS, rows, width), bf16),
            pltpu.VMEM((2, LEVELS, cap, width), bf16),
            pltpu.VMEM((2, LEVELS, rows, width), bf16),
            pltpu.VMEM((rows, 2 * hid + 2 * common), f32),
            pltpu.VMEM((rows, 2 * hid), f32),
            pltpu.VMEM((3, hid, 2 * LEVELS * rows), bf16),
            pltpu.VMEM((3, common, LEVELS * rows), bf16),
            pltpu.VMEM((LEVELS, rows, width), f32),
            pltpu.VMEM((LEVELS, rows, width), f32),
            pltpu.VMEM((LEVELS, rows, width), bf16),
            pltpu.VMEM((2, LEVELS, rows, width), bf16),
            pltpu.VMEM((LEVELS, rows, width), bf16),
            pltpu.VMEM((LEVELS, rows, width), bf16),
            pltpu.VMEM((rows, width), bf16),
            pltpu.VMEM((rows, width), bf16),
            pltpu.VMEM((cap, width), bf16),
            pltpu.VMEM((rows, width), bf16),
            pltpu.VMEM((group, 2) + shared, f32),
            pltpu.VMEM((group, 2) + shared, bf16),
            pltpu.VMEM((group, 2) + shared, bf16),
            pltpu.VMEM(shared, bf16),
            pltpu.VMEM(shared, bf16),
            dma((10,)),
            dma((count - 1,)),
            dma((count - 1,)),
            dma((count - 1,)),
            dma((count - 1,)),
            dma((2, 2, LEVELS, PIECES)),
            dma((2, LEVELS, PIECES)),
            dma((2, LEVELS, PIECES)),
            dma((2, LEVELS, PIECES)),
            dma((LEVELS, PIECES)),
            dma((2, LEVELS, PIECES)),
            dma((LEVELS, PIECES)),
            dma((LEVELS, PIECES)),
            dma((PIECES,)),
            dma((PIECES,)),
            dma((PIECES,)),
            dma((PIECES,)),
            dma((group,)),
            dma((group,)),
            dma((2,)),
        ],
        compiler_params=pltpu.CompilerParams(
            collective_id=0, has_side_effects=True, vmem_limit_bytes=55 * 2**20
        ),
    )(tokens, cotangent, ids, weights, *experts, *commons)


def flush_kernel(count, *refs):
    copies = [
        pltpu.make_async_copy(refs[i], refs[count + i], refs[2 * count].at[i]) for i in range(count)
    ]
    for copy in copies:
        copy.start()
    for copy in copies:
        copy.wait()


def flush(*held):
    count = len(held)
    return pl.pallas_call(
        functools.partial(flush_kernel, count),
        out_shape=tuple(jax.ShapeDtypeStruct(x.shape, x.dtype) for x in held),
        in_specs=[pl.BlockSpec(memory_space=pltpu.VMEM)] * count,
        out_specs=(pl.BlockSpec(memory_space=pl.ANY),) * count,
        scratch_shapes=[pltpu.SemaphoreType.DMA((count,))],
        compiler_params=pltpu.CompilerParams(vmem_limit_bytes=2**20),
    )(*held)


def gathered_shards(
    tokens,
    expert_ids,
    route_weights,
    cotangent,
    gate_weight,
    up_weight,
    down_weight,
    shared_gate,
    shared_up,
    shared_down,
):
    count, group = lax.axis_size("ep"), lax.axis_size("tp")
    held = layer(
        tokens,
        cotangent,
        expert_ids.T,
        route_weights.T,
        (gate_weight[0], up_weight[0], down_weight[0]),
        (shared_gate, shared_up, shared_down),
        count,
        group,
        3 * tokens.shape[0] * expert_ids.shape[1] // (2 * count),
    )
    token_grad, route_grad, gate_grad, up_grad, down_grad, shared_sum = flush(*held)
    return (
        token_grad,
        route_grad.T,
        gate_grad[None],
        up_grad[None],
        down_grad[None],
        jnp.transpose(shared_sum, (1, 0, 2)),
    )


def shards(tokens, expert_ids, *rest):
    dense = 2 * LEVELS == lax.axis_size("ep") <= 2 * expert_ids.shape[1]
    return (gathered_shards if dense else exchanged_shards)(tokens, expert_ids, *rest)


def solution(mesh):
    in_specs = (
        P(("ep", "tp"), None),
        P(("ep", "tp"), None),
        P(("ep", "tp"), None),
        P(("ep", "tp"), None),
        P(("ep", "tp"), None, None),
        P(("ep", "tp"), None, None),
        P(("ep", "tp"), None, None),
        P(),
        P(),
        P(),
    )
    out_specs = (
        P(("ep", "tp"), None),
        P(("ep", "tp"), None),
        P(("ep", "tp"), None, None),
        P(("ep", "tp"), None, None),
        P(("ep", "tp"), None, None),
        P(("ep", "tp"), None, None),
    )
    return jax.shard_map(shards, mesh=mesh, in_specs=in_specs, out_specs=out_specs, check_vma=False)
```
